32 devices in a mesh: sp: 8 (over z, x), tp: 4 (over y, core).
Axes of the slice: x: 2, y: 2, z: 4, core: 2. Of those that a mesh axis runs over, the one named last changes fastest.
Arguments:
- hidden_states: bfloat16 [6144, 4096], P('sp'), may hold values from -60 to 60
- w_conv_b: bfloat16 [4096, 2048], P(None, 'tp'), may hold values from -0.09375 to 0.09375
- w_conv_c: bfloat16 [4096, 2048], P(None, 'tp'), may hold values from -0.09375 to 0.09375
- w_conv_h: bfloat16 [4096, 2048], P(None, 'tp'), may hold values from -0.09375 to 0.09375
- conv_taps: bfloat16 [3, 2048], P(None, 'tp'), may hold values from -3.5 to 3.5
- w_query: bfloat16 [4096, 2048], P(None, 'tp'), may hold values from -0.15625 to 0.15625
- w_key: bfloat16 [4096, 2048], P(None, 'tp'), may hold values from -0.09375 to 0.09375
- w_value: bfloat16 [4096, 2048], P(None, 'tp'), may hold values from -0.09375 to 0.09375
- lambdas: float32 [16], P('tp'), may hold values from 0.3 to 0.8
- head_gain: bfloat16 [128], replicated, may hold values from 0.099609375 to 1.8984375
- w_out_conv: bfloat16 [2048, 4096], P('tp'), may hold values from -1 to 1
- w_out_attn: bfloat16 [2048, 4096], P('tp'), may hold values from -1 to 1
- out_gain: bfloat16 [4096], replicated, may hold values from 0.099609375 to 1.8984375
Outputs:
- mixed: bfloat16 [6144, 4096], P('sp', 'tp')
The draws below stay inside these ranges and needn't reach their ends.
All inputs are finite; a program needn't handle non-finite values.
Results may differ from the reference program's by a relative error of at most 0.023.
Values may be sent and summed in bfloat16 or wider, within the bound.
A program may use at most 192 MiB of HBM per device.

```python
import jax
import jax.numpy as jnp
from jax import lax

D = 4096
HEADS = 16
QK = 64
CONV = 2048
TAPS = 3
TOK_DEV = 768
VD = 128
TOKENS = 6144
N_TP = 4


def draw_hidden_states(key, part):
    values = jnp.clip(jax.random.normal(key, (TOKENS, D), jnp.float32), -6.0, 6.0)
    return jnp.clip(values, -60.0, 60.0).astype(jnp.bfloat16)


def rising_columns(key, row_count):
    columns = jnp.arange(D, dtype=jnp.float32) / D
    base = jnp.clip(jax.random.normal(key, (row_count, D), jnp.float32), -6.0, 6.0)
    ramp = 3.0 ** columns
    values = base * ramp[None, :] * (CONV + HEADS * VD) ** (-0.5)
    return jnp.clip(values, -1.0, 1.0).astype(jnp.bfloat16)


def draw_w_out_conv(key, part):
    return rising_columns(jax.random.fold_in(key, 11), CONV)


def draw_w_out_attn(key, part):
    return rising_columns(jax.random.fold_in(key, 13), HEADS * VD)


def block_scale(own_key, shape, cuts, smallest, high):
    gain = 1.0
    for position, shards_of in cuts:
        draws = jax.random.uniform(jax.random.fold_in(jax.random.fold_in(own_key, 6), position), (shards_of,), jnp.float32, smallest / len(cuts), high / len(cuts))
        gain = gain * jnp.repeat(jnp.exp(draws), shape[position] // shards_of).reshape((-1,) + (1,) * (len(shape) - 1 - position))
    return gain


def normal_values(key, shape, width, most, cuts=(), kind=jnp.bfloat16):
    values = width * jax.random.normal(key, shape, jnp.float32)
    if cuts:
        values = values * block_scale(key, shape, cuts, -0.22, 0.18)
    return jnp.clip(values, -most, most).astype(kind)


def setup_inputs(seed: int = 0) -> dict:
    splits = jax.random.split(jax.random.key(seed), 14)
    return {
        "hidden_states": draw_hidden_states(jax.random.fold_in(splits[13], 71), 0),
        "w_conv_b": normal_values(splits[1], (D, CONV), D ** -0.5, 0.09375, ((1, 4),)),
        "w_conv_c": normal_values(splits[2], (D, CONV), D ** -0.5, 0.09375, ((1, 4),)),
        "w_conv_h": normal_values(splits[3], (D, CONV), D ** -0.5, 0.09375, ((1, 4),)),
        "conv_taps": normal_values(splits[4], (TAPS, CONV), TAPS ** -0.5, 3.5, ((1, 4),)),
        "w_query": normal_values(splits[5], (D, HEADS * 2 * QK), (D // 3) ** -0.5, 0.15625, ((1, 4),)),
        "w_key": normal_values(splits[6], (D, HEADS * 2 * QK), D ** -0.5, 0.09375, ((1, 4),)),
        "w_value": normal_values(splits[7], (D, HEADS * VD), D ** -0.5, 0.09375, ((1, 4),)),
        "lambdas": jnp.clip(0.3 + 0.5 * jax.random.uniform(splits[8], (HEADS,), jnp.float32) ** block_scale(splits[8], (HEADS,), ((0, 4),), -0.2, 0.2), 0.3, 0.8),
        "head_gain": jnp.clip(1.0 + 0.18 * jax.random.normal(splits[9], (VD,), jnp.float32), 0.099609375, 1.8984375).astype(jnp.bfloat16),
        "w_out_conv": draw_w_out_conv(jax.random.fold_in(splits[13], 71), 0),
        "w_out_attn": draw_w_out_attn(jax.random.fold_in(splits[13], 71), 0),
        "out_gain": jnp.clip(1.0 + 0.18 * jax.random.normal(splits[12], (D,), jnp.float32), 0.099609375, 1.8984375).astype(jnp.bfloat16),
    }


def rotate(values, positions):
    inverse = 1.0 / 10000.0 ** (jnp.arange(0, QK, 2, dtype=jnp.float32) / QK)
    angles = positions[:, None] * inverse[None, :]
    angles = jnp.concatenate([angles, angles], axis=-1)
    cosine = jnp.cos(angles)[:, None, None, :]
    sine = jnp.sin(angles)[:, None, None, :]
    first_half, second_half = jnp.split(values, 2, axis=-1)
    return values * cosine + jnp.concatenate([-second_half, first_half], axis=-1) * sine

def reference(hidden_states, w_conv_b, w_conv_c, w_conv_h, conv_taps, w_query, w_key, w_value, lambdas, head_gain, w_out_conv, w_out_attn, out_gain):

    def project(weight):
        return jnp.dot(hidden_states, weight, preferred_element_type=jnp.float32).astype(jnp.bfloat16)
    u_b = project(w_conv_b)
    u_c = project(w_conv_c)
    u_h = project(w_conv_h)
    gated = u_c.astype(jnp.float32) * u_h.astype(jnp.float32)
    padded = jnp.concatenate([jnp.zeros((TAPS - 1, CONV), jnp.float32), gated], axis=0)
    taps_f = conv_taps.astype(jnp.float32)
    convolved = jnp.zeros((TOKENS, CONV), jnp.float32)
    for tap in range(TAPS):
        convolved = convolved + taps_f[tap][None, :] * padded[tap:tap + TOKENS]
    conv_out = (u_b.astype(jnp.float32) * convolved).astype(jnp.bfloat16)
    positions = jnp.arange(TOKENS, dtype=jnp.float32)
    query = rotate(project(w_query).reshape(TOKENS, HEADS, 2, QK).astype(jnp.float32), positions).astype(jnp.bfloat16)
    keys = rotate(project(w_key).reshape(TOKENS, HEADS, 2, QK).astype(jnp.float32), positions).astype(jnp.bfloat16)
    values = project(w_value).reshape(TOKENS, HEADS, VD)
    gain_f = head_gain.astype(jnp.float32)
    key_pos = jnp.arange(TOKENS, dtype=jnp.int32)

    def one_head(args):
        head_query, head_keys, head_values, weight_two = args
        keys_f = head_keys.astype(jnp.float32)
        values_f = head_values.astype(jnp.float32)

        def one_block(block_index):
            first = (block_index * TOK_DEV).astype(jnp.int32)
            block_query = lax.dynamic_slice_in_dim(head_query, first, TOK_DEV, 0).astype(jnp.float32)
            scores = jnp.einsum('qcd,kcd->cqk', block_query, keys_f) * QK ** (-0.5)
            query_pos = first + jnp.arange(TOK_DEV, dtype=jnp.int32)
            visible = key_pos[None, :] <= query_pos[:, None]
            scores = jnp.where(visible[None], scores, -jnp.inf)
            top = lax.optimization_barrier(jnp.max(scores, axis=-1, keepdims=True))
            weights = jnp.exp(scores - top)
            denom = lax.optimization_barrier(jnp.sum(weights, axis=-1))
            rounded = lax.optimization_barrier(weights.astype(jnp.bfloat16)).astype(jnp.float32)
            numer = jnp.einsum('cqk,ke->cqe', rounded, values_f)
            diff = numer[0] / denom[0][:, None] - weight_two * numer[1] / denom[1][:, None]
            normed = diff * lax.rsqrt(lax.optimization_barrier(jnp.mean(diff * diff, axis=-1, keepdims=True)) + 1e-05) * gain_f[None, :]
            return normed.astype(jnp.bfloat16)
        blocks = lax.map(one_block, jnp.arange(TOKENS // TOK_DEV, dtype=jnp.int32))
        return blocks.reshape(TOKENS, VD)
    per_head = lax.map(one_head, (query.transpose(1, 0, 2, 3), keys.transpose(1, 0, 2, 3), values.transpose(1, 0, 2), lambdas))
    attn_out = per_head.transpose(1, 0, 2).reshape(TOKENS, HEADS * VD)
    conv_width = CONV // N_TP
    attn_width = HEADS * VD // N_TP
    total = jnp.zeros((TOKENS, D), jnp.float32)
    for block in range(N_TP):
        term = jnp.dot(conv_out[:, block * conv_width:(block + 1) * conv_width], w_out_conv[block * conv_width:(block + 1) * conv_width], preferred_element_type=jnp.float32)
        term = term + jnp.dot(attn_out[:, block * attn_width:(block + 1) * attn_width], w_out_attn[block * attn_width:(block + 1) * attn_width], preferred_element_type=jnp.float32)
        total = total + lax.optimization_barrier(term.astype(jnp.bfloat16)).astype(jnp.float32)
    mix = total.astype(jnp.bfloat16).astype(jnp.float32)
    mean_value = lax.optimization_barrier(jnp.mean(mix, axis=-1, keepdims=True))
    variance = lax.optimization_barrier(jnp.mean(mix * mix, axis=-1, keepdims=True)) - mean_value * mean_value
    normed = (mix - mean_value) * lax.rsqrt(variance + 1e-05) * out_gain.astype(jnp.float32)[None, :]
    return normed.astype(jnp.bfloat16)
```

```python
import functools
import math

import jax
import jax.numpy as jnp
from jax import lax
from jax.experimental import pallas as pl
from jax.experimental.pallas import tpu as pltpu
from jax.sharding import PartitionSpec as P

QK = 64
VD = 128
TILE = 256
HEAD_ROWS = 16
NEG_LARGE = -1e30
VMEM_LIMIT = 62 * 1024 * 1024
MESH = pl.DeviceIdType.MESH


def mixer_kernel(
    n,
    tp,
    x_ref,
    cos_ref,
    sin_ref,
    taps_ref,
    lam_ref,
    gain_ref,
    wq_ref,
    wk_ref,
    wv_ref,
    wb_ref,
    wc_ref,
    wh_ref,
    conv_ref,
    attn_ref,
    wbuf,
    q_own,
    kv_own,
    q_all,
    kv_all,
    out_own,
    m_ref,
    l_ref,
    acc_ref,
    lam_all,
    rim_own,
    rim_in,
    first_g,
    first_b,
    w_sem,
    send_q,
    send_kv,
    recv_q,
    recv_kv,
    send_fwd,
    recv_fwd,
    send_o,
    recv_o,
    small_send,
    small_recv,
    lam_sem,
):
    j, t = lax.axis_index("sp"), lax.axis_index("tp")
    c, y = t % 2, t // 2
    tok = x_ref.shape[0]
    heads = q_own.shape[0]
    channels = conv_ref.shape[1]
    half = n // 2
    repeat = half // heads
    parts = 2 * repeat
    rows = tok // parts
    per = TILE // VD
    pairs, tiles = heads // per, channels // TILE

    barrier = pltpu.get_barrier_semaphore()

    @pl.loop(0, n)
    def _(a):
        for e in range(2):

            @pl.when(jnp.logical_or(a != j, c != e))
            def _():
                pl.semaphore_signal(
                    barrier, inc=1, device_id=(a, y * 2 + e), device_id_type=MESH
                )

    qkv_refs, conv_refs = (wq_ref, wk_ref, wv_ref), (wb_ref, wc_ref, wh_ref)

    def load(refs, index, slot):
        for w, ref in enumerate(refs):
            pltpu.make_async_copy(
                ref.at[:, pl.ds(pl.multiple_of(index * TILE, TILE), TILE)],
                wbuf.at[slot, w],
                w_sem.at[slot, w],
            ).start()

    def loaded(refs, slot):
        for w, ref in enumerate(refs):
            pltpu.make_async_copy(
                ref.at[:, pl.ds(0, TILE)], wbuf.at[slot, w], w_sem.at[slot, w]
            ).wait()

    def pair_of(g):
        return (g + j) % pairs

    load(qkv_refs, pair_of(0), 0)
    pl.semaphore_wait(barrier, 2 * n - 1)

    sibling = (j, y * 2 + 1 - c)
    lam_copy = pltpu.make_async_remote_copy(
        src_ref=lam_ref,
        dst_ref=lam_all.at[c],
        send_sem=small_send.at[0],
        recv_sem=small_recv.at[0],
        device_id=sibling,
        device_id_type=MESH,
    )
    lam_copy.start()
    lam_local = pltpu.make_async_copy(lam_ref, lam_all.at[c], lam_sem)
    lam_local.start()

    def part_of(block, rep, core):
        part = rep * 2 + core
        return jnp.where(block % 2 == 0, part, parts - 1 - part)

    def put(src, dst, send_sem, recv_sem, device, here):
        @pl.when(here)
        def _():
            pltpu.make_async_copy(src, dst, recv_sem).start()

        @pl.when(jnp.logical_not(here))
        def _():
            pltpu.make_async_remote_copy(
                src_ref=src,
                dst_ref=dst,
                send_sem=send_sem,
                recv_sem=recv_sem,
                device_id=device,
                device_id_type=MESH,
            ).start()

    def put_done(src, send_sem, here):
        @pl.when(jnp.logical_not(here))
        def _():
            pltpu.make_async_remote_copy(
                src_ref=src,
                dst_ref=src,
                send_sem=send_sem,
                recv_sem=send_sem,
                device_id=sibling,
                device_id_type=MESH,
            ).wait_send()

    def arrived(dst, recv_sem):
        pltpu.make_async_copy(dst, dst, recv_sem).wait()

    lane = lax.broadcasted_iota(jnp.int32, (tok, VD), 1)
    low = lane % QK < QK // 2
    fold = QK ** (-0.5) * math.log2(math.e)

    def rotate(values):
        values = values.astype(jnp.float32)
        partner = jnp.where(
            low, pltpu.roll(values, VD - QK // 2, 1), pltpu.roll(values, QK // 2, 1)
        )
        return values * cos_ref[...] + partner * sin_ref[...]

    def project(slot, w):
        return jnp.dot(
            x_ref[...], wbuf[slot, w], preferred_element_type=jnp.float32
        ).astype(jnp.bfloat16)

    @pl.loop(0, pairs)
    def _(g):
        slot = g % 2

        @pl.when(g + 1 < pairs)
        def _():
            load(qkv_refs, pair_of(g + 1), 1 - slot)

        @pl.when(g + 1 == pairs)
        def _():
            load(conv_refs, 0, 1 - slot)

        loaded(qkv_refs, slot)
        pair = pair_of(g)
        k = project(slot, 1)
        for p in range(per):
            kv_own[0, pair * per + p] = rotate(k[:, p * VD : (p + 1) * VD]).astype(jnp.bfloat16)
        v = project(slot, 2)
        for p in range(per):
            kv_own[1, pair * per + p] = v[:, p * VD : (p + 1) * VD]
        q = project(slot, 0)
        for p in range(per):
            q_own[pair * per + p] = (rotate(q[:, p * VD : (p + 1) * VD]) * fold).astype(
                jnp.bfloat16
            )
        for p in range(per):
            head = pair * per + p
            for r in range(repeat):
                local = head * repeat + r
                s = c * half + local
                for e in range(2):
                    here = jnp.logical_and(s == j, c == e)
                    first = pl.multiple_of(part_of(j, r, e) * rows, 16)
                    device = (s, y * 2 + e)
                    put(
                        kv_own.at[e, head],
                        kv_all.at[e, j],
                        send_kv.at[local * 2 + e],
                        recv_kv.at[j],
                        device,
                        here,
                    )
                    put(
                        q_own.at[head, pl.ds(first, rows)],
                        q_all.at[j],
                        send_q.at[local * 2 + e],
                        recv_q.at[j],
                        device,
                        here,
                    )

    taps = taps_ref[...].astype(jnp.float32)

    @pl.loop(0, tiles)
    def _(g):
        slot = (pairs + g) % 2

        @pl.when(g + 1 < tiles)
        def _():
            load(conv_refs, g + 1, 1 - slot)

        loaded(conv_refs, slot)
        cols = pl.ds(pl.multiple_of(g * TILE, TILE), TILE)
        gated = project(slot, 1).astype(jnp.float32) * project(slot, 2).astype(jnp.float32)
        row = lax.broadcasted_iota(jnp.int32, gated.shape, 0)
        back_one = jnp.where(row == 0, 0.0, pltpu.roll(gated, 1, 0))
        back_two = jnp.where(row < 2, 0.0, pltpu.roll(gated, 2, 0))
        tap = taps_ref[:, cols].astype(jnp.float32)
        conv = tap[0:1] * back_two + tap[1:2] * back_one + tap[2:3] * gated
        gate = project(slot, 0).astype(jnp.float32)
        conv_ref[:, cols] = (gate * conv).astype(jnp.bfloat16)
        first_g[:, cols] = gated[:HEAD_ROWS]
        first_b[:, cols] = gate[:HEAD_ROWS]
        rim_own[:, cols] = gated[tok - 8 :]

    rim_copy = pltpu.make_async_remote_copy(
        src_ref=rim_own,
        dst_ref=rim_in,
        send_sem=small_send.at[1],
        recv_sem=small_recv.at[1],
        device_id=(jnp.minimum(j + 1, n - 1), t),
        device_id_type=MESH,
    )

    @pl.when(j + 1 < n)
    def _():
        rim_copy.start()

    lam_copy.wait()
    lam_local.wait()

    side = j // half
    head_at = (j % half) // repeat
    rep_at = j % repeat
    owner_tp = y * 2 + side
    lam = lam_all[side, pl.ds(head_at, 1)]
    gain = gain_ref[...].astype(jnp.float32)
    block_lane = lax.broadcasted_iota(jnp.int32, (rows, VD), 1)

    def forward(block):
        arrived(kv_all.at[c, block], recv_kv.at[block])
        pltpu.make_async_remote_copy(
            src_ref=kv_all.at[c, block],
            dst_ref=kv_all.at[c, block],
            send_sem=send_fwd.at[block],
            recv_sem=recv_fwd.at[block],
            device_id=sibling,
            device_id_type=MESH,
        ).start()

    def attend(block, kb, both, part, masked):
        k, v = kv_all[0, kb], kv_all[1, kb]
        s = lax.dot_general(both, k, (((1,), (1,)), ((), ())), preferred_element_type=jnp.float32)
        if masked:
            r = part * rows + lax.broadcasted_iota(jnp.int32, s.shape, 0) % rows
            s = jnp.where(lax.broadcasted_iota(jnp.int32, s.shape, 1) <= r, s, NEG_LARGE)
        slabs = [s[:, b * VD : (b + 1) * VD] for b in range(tok // VD)]
        old = m_ref[block]
        top = functools.reduce(jnp.maximum, slabs)
        new = jnp.maximum(old, jnp.max(top, axis=1, keepdims=True))
        factor = jnp.exp2(old - new)
        total = l_ref[block] * factor
        weights = []
        for slab in slabs:
            w = jnp.exp2(slab - new)
            total = total + w
            weights.append(w.astype(jnp.bfloat16))
        m_ref[block] = new
        l_ref[block] = total
        acc_ref[block] = acc_ref[block] * factor + jnp.dot(
            jnp.concatenate(weights, axis=1), v, preferred_element_type=jnp.float32
        )

    def home(block, part):
        return attn_ref.at[
            pl.ds(pl.multiple_of(part * rows, 16), rows),
            pl.ds(pl.multiple_of(head_at * VD, VD), VD),
        ]

    @pl.loop(0, 3 * half)
    def _(step):
        phase = step // half
        turn = (step + j) % half
        group = jnp.where(phase == 0, side, jnp.where(phase == 1, 1 - side, 1))
        block = group * half + turn
        base = group * half

        @pl.when(jnp.logical_and(step % half == 0, phase < 2))
        def _():
            @pl.loop(0, half)
            def _(b):
                forward(base + b)

            @pl.loop(0, half)
            def _(b):
                arrived(q_all.at[base + b], recv_q.at[base + b])
                arrived(kv_all.at[1 - c, base + b], recv_fwd.at[base + b])

        q = q_all[block]
        zero = jnp.zeros_like(q)
        both = jnp.concatenate(
            [jnp.where(block_lane < QK, q, zero), jnp.where(block_lane < QK, zero, q)], axis=0
        )
        part = part_of(block, rep_at, c)

        @pl.when(phase < 2)
        def _():
            m_ref[block] = jnp.full(m_ref.shape[1:], NEG_LARGE, jnp.float32)
            l_ref[block] = jnp.zeros(l_ref.shape[1:], jnp.float32)
            acc_ref[block] = jnp.zeros(acc_ref.shape[1:], jnp.float32)

        @pl.loop(jnp.where(phase == 2, 0, base), jnp.where(phase == 2, half, block))
        def _(kb):
            attend(block, kb, both, part, False)

        @pl.when(phase < 2)
        def _():
            attend(block, block, both, part, True)

        @pl.when(jnp.logical_or(phase == 2, group == 0))
        def _():
            first, second = (
                acc_ref[block, span] / jnp.sum(l_ref[block, span], axis=1, keepdims=True)
                for span in (pl.ds(0, rows), pl.ds(rows, rows))
            )
            diff = first - lam * second
            norm = lax.rsqrt(jnp.mean(diff * diff, axis=1, keepdims=True) + 1e-05)
            out_own[block] = (diff * norm * gain).astype(jnp.bfloat16)
            put(
                out_own.at[block],
                home(block, part),
                send_o.at[block],
                recv_o.at[(j % half) * 2 + c],
                (block, owner_tp),
                jnp.logical_and(block == j, side == c),
            )

    @pl.when(j > 0)
    def _():
        rim_copy.wait_recv()

    before = jnp.where(j > 0, rim_in[...], 0.0)
    gated, gate = first_g[...], first_b[...]
    row = lax.broadcasted_iota(jnp.int32, gated.shape, 0)
    one, two = before[7:8], before[6:7]
    back_one = jnp.where(row == 0, one, pltpu.roll(gated, 1, 0))
    back_two = jnp.where(row == 0, two, jnp.where(row == 1, one, pltpu.roll(gated, 2, 0)))
    conv = taps[0:1] * back_two + taps[1:2] * back_one + taps[2:3] * gated
    conv_ref[:HEAD_ROWS] = (gate * conv).astype(jnp.bfloat16)

    @pl.when(j + 1 < n)
    def _():
        rim_copy.wait_send()

    @pl.loop(0, half)
    def _(local):
        head, rep = local // repeat, local % repeat
        s = c * half + local
        for e in range(2):
            here = jnp.logical_and(s == j, c == e)
            put_done(kv_own.at[e, head], send_kv.at[local * 2 + e], here)
            put_done(q_own.at[head, pl.ds(0, rows)], send_q.at[local * 2 + e], here)

    @pl.loop(0, n)
    def _(block):
        put_done(kv_all.at[c, block], send_fwd.at[block], j < 0)
        put_done(out_own.at[block], send_o.at[block], jnp.logical_and(block == j, side == c))

    @pl.loop(0, n)
    def _(piece):
        arrived(out_own.at[0], recv_o.at[piece])


def per_device(
    n,
    tp,
    hidden_states,
    w_conv_b,
    w_conv_c,
    w_conv_h,
    conv_taps,
    w_query,
    w_key,
    w_value,
    lambdas,
    head_gain,
    w_out_conv,
    w_out_attn,
    out_gain,
):
    tok, model = hidden_states.shape
    heads = w_value.shape[1] // VD
    channels = w_conv_b.shape[1]
    j, t = lax.axis_index("sp"), lax.axis_index("tp")
    c, y = t % 2, t // 2
    half = n // 2
    repeat = half // heads
    parts = 2 * repeat
    rows = tok // parts
    pair = [(a, a ^ 1) for a in range(tp)]

    inverse = 1.0 / 10000.0 ** (jnp.arange(0, QK, 2, dtype=jnp.float32) / QK)
    positions = (j * tok + jnp.arange(tok, dtype=jnp.int32)).astype(jnp.float32)
    angles = positions[:, None] * inverse[None, :]
    cos, sin = jnp.cos(angles), jnp.sin(angles)
    cos = jnp.concatenate([cos] * 4, axis=1)
    sin = jnp.concatenate([-sin, sin] * 2, axis=1)
    lam_rows = -(-heads // 8) * 8
    lam = jnp.pad(lambdas, (0, lam_rows - heads))[:, None] + jnp.zeros((1, VD), jnp.float32)

    vmem, hbm = pl.BlockSpec(memory_space=pltpu.VMEM), pl.BlockSpec(memory_space=pl.ANY)
    bf16, f32 = jnp.bfloat16, jnp.float32
    dma = pltpu.SemaphoreType.DMA
    conv_out, attn_out = pl.pallas_call(
        functools.partial(mixer_kernel, n, tp),
        out_shape=(
            jax.ShapeDtypeStruct((tok, channels), bf16),
            jax.ShapeDtypeStruct((tok, heads * VD), bf16),
        ),
        in_specs=[vmem] * 6 + [hbm] * 6,
        out_specs=(vmem, vmem),
        scratch_shapes=[
            pltpu.VMEM((2, 3, model, TILE), bf16),
            pltpu.VMEM((heads, tok, VD), bf16),
            pltpu.VMEM((2, heads, tok, VD), bf16),
            pltpu.VMEM((n, rows, VD), bf16),
            pltpu.VMEM((2, n, tok, VD), bf16),
            pltpu.VMEM((n, rows, VD), bf16),
            pltpu.VMEM((n, 2 * rows, VD), f32),
            pltpu.VMEM((n, 2 * rows, VD), f32),
            pltpu.VMEM((n, 2 * rows, VD), f32),
            pltpu.VMEM((2, lam_rows, VD), f32),
            pltpu.VMEM((8, channels), f32),
            pltpu.VMEM((8, channels), f32),
            pltpu.VMEM((HEAD_ROWS, channels), f32),
            pltpu.VMEM((HEAD_ROWS, channels), f32),
            dma((2, 3)),
            dma((n,)),
            dma((n,)),
            dma((n,)),
            dma((n,)),
            dma((n,)),
            dma((n,)),
            dma((n,)),
            dma((n,)),
            dma((2,)),
            dma((2,)),
            dma,
        ],
        compiler_params=pltpu.CompilerParams(
            vmem_limit_bytes=VMEM_LIMIT, collective_id=0, has_side_effects=True
        ),
        cost_estimate=pl.CostEstimate(
            flops=12 * tok * model * channels + 4 * n * n * rows * tok * VD,
            bytes_accessed=2 * model * (tok + 6 * channels),
            transcendentals=0,
        ),
        name="mixer",
    )(
        hidden_states,
        cos,
        sin,
        conv_taps,
        lam,
        head_gain[None],
        w_query,
        w_key,
        w_value,
        w_conv_b,
        w_conv_c,
        w_conv_h,
    )

    ranks = tp // 2
    width = model // tp

    def halves(rank, conv_rows, attn_rows):
        cols = lambda w: lax.dynamic_slice_in_dim(w, rank * 2 * width, 2 * width, 1)
        value = jnp.dot(
            conv_rows, cols(w_out_conv), preferred_element_type=jnp.float32
        ) + jnp.dot(attn_rows, cols(w_out_attn), preferred_element_type=jnp.float32)
        value = value.astype(jnp.bfloat16)
        own = jnp.where(c == 0, value[:, :width], value[:, width:])
        away = jnp.where(c == 0, value[:, width:], value[:, :width])
        return own, away

    def pair_sum(own, away):
        return own.astype(jnp.float32) + lax.ppermute(away, "tp", pair).astype(jnp.float32)

    arriving, totals = [], []
    chunk = tok // 2
    for step in range(1, ranks):
        onward = [(a, (a // 2 + step) % ranks * 2 + a % 2) for a in range(tp)]
        blocks = []
        for first in (0, chunk):
            rows_of = slice(first, first + chunk)
            own, away = halves((y + step) % ranks, conv_out[rows_of], attn_out[rows_of])
            total = pair_sum(own, away).astype(jnp.bfloat16)
            totals.append(total)
            blocks.append(lax.ppermute(total, "tp", onward))
        arriving.append(blocks)
    conv_late, attn_late, *_ = lax.optimization_barrier((conv_out, attn_out, *totals))
    own, away = halves(y, conv_late, attn_late)
    if arriving:
        own, away, arriving[0][0] = lax.optimization_barrier((own, away, arriving[0][0]))
    mix = pair_sum(own, away)
    for blocks in arriving:
        mix = mix + jnp.concatenate(blocks, axis=0).astype(jnp.float32)
    mix_f = mix.astype(jnp.bfloat16).astype(jnp.float32)
    total_sum, total_squares = lax.psum(
        (jnp.sum(mix_f, axis=-1), jnp.sum(mix_f * mix_f, axis=-1)), "tp"
    )
    mean_value = (total_sum / model)[:, None]
    variance = (total_squares / model)[:, None] - mean_value * mean_value
    own_gain = lax.dynamic_slice_in_dim(out_gain, t * width, width, 0).astype(jnp.float32)
    return ((mix_f - mean_value) * lax.rsqrt(variance + 1e-05) * own_gain[None, :]).astype(
        jnp.bfloat16
    )


def solution(mesh):
    n, tp = mesh.shape["sp"], mesh.shape["tp"]
    return jax.shard_map(
        functools.partial(per_device, n, tp),
        mesh=mesh,
        in_specs=(
            P("sp", None),
            P(None, "tp"),
            P(None, "tp"),
            P(None, "tp"),
            P(None, "tp"),
            P(None, "tp"),
            P(None, "tp"),
            P(None, "tp"),
            P("tp"),
            P(),
            P("tp", None),
            P("tp", None),
            P(),
        ),
        out_specs=P("sp", "tp"),
        check_vma=False,
    )
```

```python
import functools
import math

import jax
import jax.numpy as jnp
import numpy as np
from jax import lax
from jax.experimental import pallas as pl
from jax.experimental.pallas import tpu as pltpu
from jax.sharding import PartitionSpec as P

QK = 64
VD = 128
TILE = 256
SPAN = 256
HEAD_ROWS = 16
NEG_LARGE = -1e30
VMEM_LIMIT = 67_000_000
MESH = pl.DeviceIdType.MESH
BF16, F32 = jnp.bfloat16, jnp.float32


def mixer_kernel(
    n,
    tp,
    turn_ref,
    base_ref,
    taps_ref,
    lam_ref,
    gain_ref,
    out_gain_ref,
    x_hbm,
    wq_ref,
    wk_ref,
    wv_ref,
    wb_ref,
    wc_ref,
    wh_ref,
    w_conv_ref,
    w_attn_ref,
    out_ref,
    x_ref,
    cos_ref,
    sin_ref,
    wbuf,
    q_own,
    kv_own,
    q_all,
    kv_all,
    out_own,
    m_ref,
    l_ref,
    acc_ref,
    lam_all,
    rim_own,
    rim_in,
    first_g,
    first_b,
    conv_chip,
    wc_all,
    wa_all,
    part_out,
    part_in,
    attn_all,
    total_ref,
    stats,
    x_sem,
    w_sem,
    send_q,
    send_kv,
    recv_q,
    recv_kv,
    send_fwd,
    recv_fwd,
    send_o,
    recv_o,
    small_send,
    small_recv,
    send_wa,
    recv_wa,
    send_wc,
    recv_wc,
    local_wc,
    send_part,
    recv_part,
    send_y,
    recv_y,
    send_s,
    recv_s,
    send_stat,
    recv_stat,
):
    j, t = lax.axis_index("sp"), lax.axis_index("tp")
    c, y = t % 2, t // 2
    ranks = tp // 2
    tok, model = x_ref.shape
    width = model // tp
    heads = q_own.shape[0]
    channels = wc_all.shape[2]
    half = n // 2
    repeat = half // heads
    parts = 2 * repeat
    rows = tok // parts
    per = TILE // VD
    pairs, tiles = heads // per, channels // TILE

    def remote(src, dst, send_sem, recv_sem, device):
        return pltpu.make_async_remote_copy(
            src_ref=src,
            dst_ref=dst,
            send_sem=send_sem,
            recv_sem=recv_sem,
            device_id=device,
            device_id_type=MESH,
        )

    sibling = (j, y * 2 + 1 - c)

    def peer(step):
        return (j, (y + step) % ranks * 2 + c)

    barrier = pltpu.get_barrier_semaphore()
    x_copy = pltpu.make_async_copy(x_hbm, x_ref, x_sem)
    x_copy.start()

    qkv_refs, conv_refs = (wq_ref, wk_ref, wv_ref), (wb_ref, wc_ref, wh_ref)

    def load(refs, index, slot):
        for w, ref in enumerate(refs):
            pltpu.make_async_copy(
                ref.at[:, pl.ds(pl.multiple_of(index * TILE, TILE), TILE)],
                wbuf.at[slot, w],
                w_sem.at[slot, w],
            ).start()

    def loaded(refs, slot, w):
        pltpu.make_async_copy(
            refs[w].at[:, pl.ds(0, TILE)], wbuf.at[slot, w], w_sem.at[slot, w]
        ).wait()

    def pair_of(g):
        return (g + j) % pairs

    load(qkv_refs, pair_of(0), 0)

    @pl.loop(0, n)
    def _(a):
        for e in range(2):

            @pl.when(jnp.logical_or(a != j, c != e))
            def _():
                pl.semaphore_signal(
                    barrier, inc=1, device_id=(a, y * 2 + e), device_id_type=MESH
                )

    @pl.loop(1, ranks)
    def _(step):
        for e in range(2):
            pl.semaphore_signal(
                barrier,
                inc=1,
                device_id=(j, (y + step) % ranks * 2 + e),
                device_id_type=MESH,
            )

    lane_row = lax.broadcasted_iota(jnp.int32, (1, VD), 1)
    cos_far, sin_far = base_ref[0, pl.ds(j, 1)], base_ref[1, pl.ds(j, 1)]
    cos_ref[...] = cos_far * turn_ref[0] - sin_far * turn_ref[1]
    sin_ref[...] = jnp.where(lane_row % QK < QK // 2, -1.0, 1.0) * (
        sin_far * turn_ref[0] + cos_far * turn_ref[1]
    )
    for h in range(heads):
        lam_all[c, h : h + 1] = jnp.full((1, VD), lam_ref[h], F32)

    pl.semaphore_wait(barrier, 2 * n - 1 + 2 * (ranks - 1))

    lam_copy = remote(lam_all.at[c], lam_all.at[c], small_send.at[0], small_recv.at[0], sibling)
    lam_copy.start()

    def wa_rows(head, source):
        return wa_all.at[pl.ds(pl.multiple_of((head * tp + source) * VD, VD), VD)]

    def wa_copy(head, target, source):
        return remote(
            w_attn_ref.at[
                pl.ds(head * VD, VD), pl.ds(pl.multiple_of(target * width, VD), width)
            ],
            wa_rows(head, source),
            send_wa.at[target, head],
            recv_wa.at[source, head],
            (j, target),
        )

    def wc_cols(rank, core):
        return w_conv_ref.at[:, pl.ds(pl.multiple_of((rank * 2 + core) * width, VD), width)]

    for head in range(heads):
        pltpu.make_async_copy(
            w_attn_ref.at[pl.ds(head * VD, VD), pl.ds(pl.multiple_of(t * width, VD), width)],
            wa_rows(head, t),
            recv_wa.at[t, head],
        ).start()

    @pl.loop(1, tp)
    def _(step):
        for head in range(heads):
            wa_copy(head, (t + step) % tp, t).start()

    @pl.loop(0, ranks)
    def _(rank):
        pltpu.make_async_copy(wc_cols(rank, c), wc_all.at[rank, c], local_wc.at[rank]).start()
        remote(
            wc_cols(rank, 1 - c), wc_all.at[rank, c], send_wc.at[rank], recv_wc.at[rank], sibling
        ).start()

    def part_of(block, rep, core):
        part = rep * 2 + core
        return jnp.where(block % 2 == 0, part, parts - 1 - part)

    def put(src, dst, send_sem, recv_sem, device, here):
        @pl.when(here)
        def _():
            pltpu.make_async_copy(src, dst, recv_sem).start()

        @pl.when(jnp.logical_not(here))
        def _():
            remote(src, dst, send_sem, recv_sem, device).start()

    def sent(src, send_sem):
        remote(src, src, send_sem, send_sem, sibling).wait_send()

    def put_done(src, send_sem, here):
        @pl.when(jnp.logical_not(here))
        def _():
            sent(src, send_sem)

    def arrived(dst, recv_sem):
        pltpu.make_async_copy(dst, dst, recv_sem).wait()

    lane = lax.broadcasted_iota(jnp.int32, (tok, VD), 1)
    low = lane % QK < QK // 2
    fold = QK ** (-0.5) * math.log2(math.e)

    def rotate(values):
        values = values.astype(F32)
        partner = jnp.where(
            low, pltpu.roll(values, VD - QK // 2, 1), pltpu.roll(values, QK // 2, 1)
        )
        return values * cos_ref[...] + partner * sin_ref[...]

    def project(slot, w):
        return jnp.dot(x_ref[...], wbuf[slot, w], preferred_element_type=F32).astype(BF16)

    x_copy.wait()

    @pl.loop(0, pairs)
    def _(g):
        slot = g % 2

        @pl.when(g + 1 < pairs)
        def _():
            load(qkv_refs, pair_of(g + 1), 1 - slot)

        @pl.when(g + 1 == pairs)
        def _():
            load(conv_refs, 0, 1 - slot)

        pair = pair_of(g)

        def send_kv_of(e):
            for p in range(per):
                head = pair * per + p
                for r in range(repeat):
                    local = head * repeat + r
                    s = c * half + local
                    put(
                        kv_own.at[e, head],
                        kv_all.at[e, j],
                        send_kv.at[local * 2 + e],
                        recv_kv.at[j],
                        (s, y * 2 + e),
                        jnp.logical_and(s == j, c == e),
                    )

        loaded(qkv_refs, slot, 1)
        k = project(slot, 1)
        for p in range(per):
            kv_own[0, pair * per + p] = rotate(k[:, p * VD : (p + 1) * VD]).astype(BF16)
        loaded(qkv_refs, slot, 2)
        send_kv_of(0)
        v = project(slot, 2)
        for p in range(per):
            kv_own[1, pair * per + p] = v[:, p * VD : (p + 1) * VD]
        loaded(qkv_refs, slot, 0)
        send_kv_of(1)
        q = project(slot, 0)
        for p in range(per):
            q_own[pair * per + p] = (rotate(q[:, p * VD : (p + 1) * VD]) * fold).astype(BF16)
        for p in range(per):
            head = pair * per + p
            for r in range(repeat):
                local = head * repeat + r
                s = c * half + local
                for e in range(2):
                    first = pl.multiple_of(part_of(j, r, e) * rows, 16)
                    put(
                        q_own.at[head, pl.ds(first, rows)],
                        q_all.at[j],
                        send_q.at[local * 2 + e],
                        recv_q.at[j],
                        (s, y * 2 + e),
                        jnp.logical_and(s == j, c == e),
                    )

    @pl.loop(0, tiles)
    def _(g):
        slot = (pairs + g) % 2

        @pl.when(g + 1 < tiles)
        def _():
            load(conv_refs, g + 1, 1 - slot)

        for w in range(3):
            loaded(conv_refs, slot, w)
        cols = pl.ds(pl.multiple_of(g * TILE, TILE), TILE)
        gated = project(slot, 1).astype(F32) * project(slot, 2).astype(F32)
        row = lax.broadcasted_iota(jnp.int32, gated.shape, 0)
        back_one = jnp.where(row == 0, 0.0, pltpu.roll(gated, 1, 0))
        back_two = jnp.where(row < 2, 0.0, pltpu.roll(gated, 2, 0))
        tap = taps_ref[:, cols].astype(F32)
        conv = tap[0:1] * back_two + tap[1:2] * back_one + tap[2:3] * gated
        gate = project(slot, 0).astype(F32)
        conv_chip[c, :, cols] = (gate * conv).astype(BF16)
        first_g[:, cols] = gated[:HEAD_ROWS]
        first_b[:, cols] = gate[:HEAD_ROWS]
        rim_own[:, cols] = gated[tok - 8 :]

    rim_copy = remote(
        rim_own, rim_in, small_send.at[1], small_recv.at[1], (jnp.minimum(j + 1, n - 1), t)
    )

    @pl.when(j + 1 < n)
    def _():
        rim_copy.start()

    lam_copy.wait()

    side = j // half
    head_at = (j % half) // repeat
    rep_at = j % repeat
    owner_tp = y * 2 + side
    lam = lam_all[side, pl.ds(head_at, 1)]
    gain = gain_ref[...].astype(F32)
    block_lane = lax.broadcasted_iota(jnp.int32, (rows, VD), 1)

    def forward(block):
        here = kv_all.at[c, block]
        arrived(here, recv_kv.at[block])
        remote(here, here, send_fwd.at[block], recv_fwd.at[block], sibling).start()

    def attend(slot, kb, both, part, masked):
        k, v = kv_all[0, kb], kv_all[1, kb]
        s = lax.dot_general(both, k, (((1,), (1,)), ((), ())), preferred_element_type=F32)
        if masked:
            r = part * rows + lax.broadcasted_iota(jnp.int32, s.shape, 0) % rows
            s = jnp.where(lax.broadcasted_iota(jnp.int32, s.shape, 1) <= r, s, NEG_LARGE)
        slabs = [s[:, b * VD : (b + 1) * VD] for b in range(tok // VD)]
        old = m_ref[slot]
        top = functools.reduce(jnp.maximum, slabs)
        new = jnp.maximum(old, jnp.max(top, axis=1, keepdims=True))
        factor = jnp.exp2(old - new)
        total = l_ref[slot] * factor
        weights = []
        for slab in slabs:
            w = jnp.exp2(slab - new)
            total = total + w
            weights.append(w.astype(BF16))
        m_ref[slot] = new
        l_ref[slot] = total
        acc_ref[slot] = acc_ref[slot] * factor + jnp.dot(
            jnp.concatenate(weights, axis=1), v, preferred_element_type=F32
        )

    def piece(head, source, part):
        return attn_all.at[
            pl.ds(pl.multiple_of(part * rows, 16), rows),
            pl.ds(pl.multiple_of((head * tp + source) * VD, VD), VD),
        ]

    def piece_of(k, core, source):
        local = (j - k) % half
        head, rep = local // repeat, local % repeat
        return local * 2 + core, piece(head, source, part_of(j, rep, core))

    def share(k):
        for core in range(2):
            index, mine = piece_of(k, core, t)
            arrived(mine, recv_o.at[index])

            @pl.loop(1, ranks)
            def _(step):
                remote(
                    mine, mine, send_y.at[step, index], recv_y.at[step, index], peer(step)
                ).start()

            remote(mine, mine, send_s.at[y, index], recv_s.at[y, index], sibling).start()

    def relay(k):
        @pl.loop(1, ranks)
        def _(step):
            rank = (y + ranks - step) % ranks
            for core in range(2):
                index, theirs = piece_of(k, core, rank * 2 + c)
                arrived(theirs, recv_y.at[step, index])
                remote(
                    theirs, theirs, send_s.at[rank, index], recv_s.at[rank, index], sibling
                ).start()

    def gathered(k):
        @pl.loop(0, ranks)
        def _(rank):
            for core in range(2):
                index, theirs = piece_of(k, core, rank * 2 + 1 - c)
                arrived(theirs, recv_s.at[rank, index])

    def fix_first_rows():
        @pl.when(j > 0)
        def _():
            rim_copy.wait_recv()

        taps = taps_ref[...].astype(F32)
        before = jnp.where(j > 0, rim_in[...], 0.0)
        gated, gate = first_g[...], first_b[...]
        row = lax.broadcasted_iota(jnp.int32, gated.shape, 0)
        one, two = before[7:8], before[6:7]
        back_one = jnp.where(row == 0, one, pltpu.roll(gated, 1, 0))
        back_two = jnp.where(row == 0, two, jnp.where(row == 1, one, pltpu.roll(gated, 2, 0)))
        conv = taps[0:1] * back_two + taps[1:2] * back_one + taps[2:3] * gated
        conv_chip[c, :HEAD_ROWS] = (gate * conv).astype(BF16)

    conv_copy = remote(
        conv_chip.at[c], conv_chip.at[c], small_send.at[2], small_recv.at[2], sibling
    )

    def conv_product(first, rank):
        span = pl.ds(first, SPAN)
        return jnp.dot(
            conv_chip[0, span], wc_all[rank, 0], preferred_element_type=F32
        ) + jnp.dot(conv_chip[1, span], wc_all[rank, 1], preferred_element_type=F32)

    def conv_parts():
        conv_copy.wait_recv()

        @pl.loop(0, ranks)
        def _(rank):
            mine = wc_all.at[rank, c]
            theirs = wc_all.at[rank, 1 - c]
            arrived(mine, local_wc.at[rank])
            arrived(theirs, recv_wc.at[rank])

        @pl.loop(1, ranks)
        def _(step):
            @pl.loop(0, tok // SPAN)
            def _(b):
                first = pl.multiple_of(b * SPAN, SPAN)
                part_out[step - 1, pl.ds(first, SPAN)] = conv_product(
                    first, (y + step) % ranks
                ).astype(BF16)

            remote(
                part_out.at[step - 1],
                part_in.at[step - 1],
                send_part.at[step - 1],
                recv_part.at[step - 1],
                peer(step),
            ).start()

    @pl.loop(0, 3 * half)
    def _(step):
        phase = step // half
        turn = (step + j) % half
        group = jnp.where(phase == 0, side, jnp.where(phase == 1, 1 - side, 1))
        block = group * half + turn
        base = group * half
        slot = jnp.where(group == 0, half, turn)

        @pl.when(jnp.logical_and(step % half == 0, phase < 2))
        def _():
            @pl.loop(0, half)
            def _(b):
                forward(base + b)

            @pl.loop(0, half)
            def _(b):
                arrived(q_all.at[base + b], recv_q.at[base + b])
                arrived(kv_all.at[1 - c, base + b], recv_fwd.at[base + b])

        @pl.when(step == 1)
        def _():
            fix_first_rows()
            conv_copy.start()

        @pl.when(step == 2)
        def _():
            conv_parts()

        @pl.when(step > 2 * half)
        def _():
            share(step - 2 * half - 1)

        @pl.when(step > 2 * half + 1)
        def _():
            relay(step - 2 * half - 2)

        q = q_all[block]
        zero = jnp.zeros_like(q)
        both = jnp.concatenate(
            [jnp.where(block_lane < QK, q, zero), jnp.where(block_lane < QK, zero, q)], axis=0
        )
        part = part_of(block, rep_at, c)

        @pl.when(phase < 2)
        def _():
            m_ref[slot] = jnp.full(m_ref.shape[1:], NEG_LARGE, F32)
            l_ref[slot] = jnp.zeros(l_ref.shape[1:], F32)
            acc_ref[slot] = jnp.zeros(acc_ref.shape[1:], F32)

        @pl.loop(jnp.where(phase == 2, 0, base), jnp.where(phase == 2, half, block))
        def _(kb):
            attend(slot, kb, both, part, False)

        @pl.when(phase < 2)
        def _():
            attend(slot, block, both, part, True)

        @pl.when(jnp.logical_or(phase == 2, group == 0))
        def _():
            first, second = (
                acc_ref[slot, span] / jnp.sum(l_ref[slot, span], axis=1, keepdims=True)
                for span in (pl.ds(0, rows), pl.ds(rows, rows))
            )
            diff = first - lam * second
            norm = lax.rsqrt(jnp.mean(diff * diff, axis=1, keepdims=True) + 1e-05)
            out_own[block] = (diff * norm * gain).astype(BF16)
            put(
                out_own.at[block],
                piece(head_at, owner_tp, part),
                send_o.at[block],
                recv_o.at[(j % half) * 2 + c],
                (block, owner_tp),
                jnp.logical_and(block == j, side == c),
            )

    share(half - 1)
    relay(half - 2)

    @pl.loop(1, ranks)
    def _(step):
        arrived(part_in.at[step - 1], recv_part.at[step - 1])

    @pl.loop(0, tok // SPAN)
    def _(b):
        first = pl.multiple_of(b * SPAN, SPAN)
        value = conv_product(first, y)
        for step in range(1, ranks):
            value = value + part_in[step - 1, pl.ds(first, SPAN)].astype(F32)
        total_ref[pl.ds(first, SPAN)] = value

    @pl.loop(0, tp)
    def _(source):
        for head in range(heads):
            arrived(wa_rows(head, source), recv_wa.at[source, head])

    def accumulate(k):
        gathered(k)
        local = (j - k) % half
        head, rep = local // repeat, local % repeat
        deep = pl.ds(pl.multiple_of(head * tp * VD, VD), tp * VD)
        for core in range(2):
            span = pl.ds(pl.multiple_of(part_of(j, rep, core) * rows, 16), rows)
            total_ref[span] = total_ref[span] + jnp.dot(
                attn_all[span, deep], wa_all[deep], preferred_element_type=F32
            )

    @pl.loop(0, half)
    def _(k):
        @pl.when(k == half - 1)
        def _():
            relay(half - 1)

        accumulate(k)

    slabs = width // VD

    @pl.loop(0, tok // SPAN)
    def _(b):
        span = pl.ds(pl.multiple_of(b * SPAN, SPAN), SPAN)
        mix = total_ref[span].astype(BF16)
        out_ref[span] = mix
        sums = jnp.zeros((SPAN, VD), F32)
        squares = jnp.zeros((SPAN, VD), F32)
        for s in range(slabs):
            slab = mix[:, s * VD : (s + 1) * VD].astype(F32)
            sums = sums + slab
            squares = squares + slab * slab
        stats[t, 0:1, span] = jnp.sum(sums.T, axis=0, keepdims=True)
        stats[t, 1:2, span] = jnp.sum(squares.T, axis=0, keepdims=True)

    def stat_copy(step):
        return remote(
            stats.at[t],
            stats.at[t],
            send_stat.at[step],
            recv_stat.at[step],
            (j, (t + step) % tp),
        )

    @pl.loop(1, tp)
    def _(step):
        stat_copy(step).start()

    own_gain = out_gain_ref[:, pl.ds(pl.multiple_of(t * width, VD), width)].astype(F32)

    @pl.loop(1, tp)
    def _(step):
        source = (t + tp - step) % tp
        arrived(stats.at[source], recv_stat.at[step])

    @pl.loop(0, tok // SPAN)
    def _(b):
        span = pl.ds(pl.multiple_of(b * SPAN, SPAN), SPAN)
        sums, squares = stats[0, 0:1, span], stats[0, 1:2, span]
        for source in range(1, tp):
            sums = sums + stats[source, 0:1, span]
            squares = squares + stats[source, 1:2, span]
        mean = sums / model
        scale = lax.rsqrt(squares / model - mean * mean + 1e-05)
        mean_cols = jnp.broadcast_to(mean, (VD, SPAN)).T
        scale_cols = jnp.broadcast_to(scale, (VD, SPAN)).T
        for s in range(slabs):
            cols = slice(s * VD, (s + 1) * VD)
            value = (out_ref[span, cols].astype(F32) - mean_cols) * scale_cols
            out_ref[span, cols] = (value * own_gain[:, cols]).astype(BF16)


    @pl.when(j + 1 < n)
    def _():
        rim_copy.wait_send()

    conv_copy.wait_send()

    @pl.loop(0, half)
    def _(local):
        head = local // repeat
        s = c * half + local
        for e in range(2):
            here = jnp.logical_and(s == j, c == e)
            put_done(kv_own.at[e, head], send_kv.at[local * 2 + e], here)
            put_done(q_own.at[head, pl.ds(0, rows)], send_q.at[local * 2 + e], here)

    @pl.loop(0, n)
    def _(block):
        sent(kv_all.at[c, block], send_fwd.at[block])
        put_done(out_own.at[block], send_o.at[block], jnp.logical_and(block == j, side == c))

        @pl.loop(1, ranks)
        def _(step):
            sent(out_own.at[0], send_y.at[step, block])

        @pl.loop(0, ranks)
        def _(rank):
            sent(out_own.at[0], send_s.at[rank, block])

    @pl.loop(1, tp)
    def _(step):
        stat_copy(step).wait_send()
        for head in range(heads):
            sent(wa_rows(head, t), send_wa.at[(t + step) % tp, head])

    @pl.loop(0, ranks)
    def _(rank):
        sent(wc_all.at[rank, c], send_wc.at[rank])

    @pl.loop(1, ranks)
    def _(step):
        sent(part_out.at[step - 1], send_part.at[step - 1])


def per_device(
    n,
    tp,
    hidden_states,
    w_conv_b,
    w_conv_c,
    w_conv_h,
    conv_taps,
    w_query,
    w_key,
    w_value,
    lambdas,
    head_gain,
    w_out_conv,
    w_out_attn,
    out_gain,
):
    tok, model = hidden_states.shape
    heads = w_value.shape[1] // VD
    channels = w_conv_b.shape[1]
    half = n // 2
    repeat = half // heads
    parts = 2 * repeat
    rows = tok // parts
    ranks = tp // 2
    width = model // tp

    inverse = 10000.0 ** (-np.arange(0, QK, 2, dtype=np.float64) / QK)
    inverse = np.tile(inverse, VD // inverse.size)[None, :]
    table = lambda angles: np.stack([np.cos(angles), np.sin(angles)]).astype(np.float32)
    turn = table(np.arange(tok)[:, None] * inverse)
    base = table(np.arange(n)[:, None] * tok * inverse)
    lam_rows = -(-heads // 8) * 8

    vmem, hbm = pl.BlockSpec(memory_space=pltpu.VMEM), pl.BlockSpec(memory_space=pl.ANY)
    smem = pl.BlockSpec(memory_space=pltpu.SMEM)
    dma = pltpu.SemaphoreType.DMA
    return pl.pallas_call(
        functools.partial(mixer_kernel, n, tp),
        out_shape=jax.ShapeDtypeStruct((tok, width), BF16),
        in_specs=[vmem] * 3 + [smem] + [vmem] * 2 + [hbm] * 9,
        out_specs=vmem,
        scratch_shapes=[
            pltpu.VMEM((tok, model), BF16),
            pltpu.VMEM((tok, VD), F32),
            pltpu.VMEM((tok, VD), F32),
            pltpu.VMEM((2, 3, model, TILE), BF16),
            pltpu.VMEM((heads, tok, VD), BF16),
            pltpu.VMEM((2, heads, tok, VD), BF16),
            pltpu.VMEM((n, rows, VD), BF16),
            pltpu.VMEM((2, n, tok, VD), BF16),
            pltpu.VMEM((n, rows, VD), BF16),
            pltpu.VMEM((half + 1, 2 * rows, VD), F32),
            pltpu.VMEM((half + 1, 2 * rows, VD), F32),
            pltpu.VMEM((half + 1, 2 * rows, VD), F32),
            pltpu.VMEM((2, lam_rows, VD), F32),
            pltpu.VMEM((8, channels), F32),
            pltpu.VMEM((8, channels), F32),
            pltpu.VMEM((HEAD_ROWS, channels), F32),
            pltpu.VMEM((HEAD_ROWS, channels), F32),
            pltpu.VMEM((2, tok, channels), BF16),
            pltpu.VMEM((ranks, 2, channels, width), BF16),
            pltpu.VMEM((heads * tp * VD, width), BF16),
            pltpu.VMEM((max(ranks - 1, 1), tok, width), BF16),
            pltpu.VMEM((max(ranks - 1, 1), tok, width), BF16),
            pltpu.VMEM((tok, heads * tp * VD), BF16),
            pltpu.VMEM((tok, width), F32),
            pltpu.VMEM((tp, 8, tok), F32),
            dma,
            dma((2, 3)),
            dma((n,)),
            dma((n,)),
            dma((n,)),
            dma((n,)),
            dma((n,)),
            dma((n,)),
            dma((n,)),
            dma((n,)),
            dma((3,)),
            dma((3,)),
            dma((tp, heads)),
            dma((tp, heads)),
            dma((ranks,)),
            dma((ranks,)),
            dma((ranks,)),
            dma((ranks,)),
            dma((ranks,)),
            dma((ranks, n)),
            dma((ranks, n)),
            dma((ranks, n)),
            dma((ranks, n)),
            dma((tp,)),
            dma((tp,)),
        ],
        compiler_params=pltpu.CompilerParams(
            vmem_limit_bytes=VMEM_LIMIT, collective_id=0, has_side_effects=True
        ),
        cost_estimate=pl.CostEstimate(
            flops=12 * tok * model * channels + 4 * n * n * rows * tok * VD,
            bytes_accessed=2 * model * (tok + 6 * channels),
            transcendentals=0,
        ),
        name="mixer",
    )(
        jnp.asarray(turn),
        jnp.asarray(base),
        conv_taps,
        lambdas,
        head_gain[None],
        out_gain[None],
        hidden_states,
        w_query,
        w_key,
        w_value,
        w_conv_b,
        w_conv_c,
        w_conv_h,
        w_out_conv,
        w_out_attn,
    )


def solution(mesh):
    n, tp = mesh.shape["sp"], mesh.shape["tp"]
    return jax.shard_map(
        functools.partial(per_device, n, tp),
        mesh=mesh,
        in_specs=(
            P("sp", None),
            P(None, "tp"),
            P(None, "tp"),
            P(None, "tp"),
            P(None, "tp"),
            P(None, "tp"),
            P(None, "tp"),
            P(None, "tp"),
            P("tp"),
            P(),
            P("tp", None),
            P("tp", None),
            P(),
        ),
        out_specs=P("sp", "tp"),
        check_vma=False,
    )
```

```python
import functools
import math

import jax
import jax.numpy as jnp
import numpy as np
from jax import lax
from jax.experimental import pallas as pl
from jax.experimental.pallas import tpu as pltpu
from jax.sharding import PartitionSpec as P

QK = 64
VD = 128
TILE = 256
SPAN = 256
RIM = 16
RING = 4
NEG_LARGE = -1e30
VMEM_LIMIT = 67_000_000
MESH = pl.DeviceIdType.MESH
BF16, F32 = jnp.bfloat16, jnp.float32


def mixer_kernel(
    n,
    tp,
    turn_ref,
    base_ref,
    taps_ref,
    lam_ref,
    gain_ref,
    x_hbm,
    wq_ref,
    wk_ref,
    wv_ref,
    wb_ref,
    wc_ref,
    wh_ref,
    w_conv_ref,
    w_attn_ref,
    out_ref,
    stat_ref,
    x_ref,
    cos_ref,
    sin_ref,
    tables,
    wbuf,
    raw_ref,
    q_own,
    kv_own,
    q_all,
    kv_all,
    out_own,
    m_ref,
    l_ref,
    acc_ref,
    lam_all,
    rim_x,
    rim_raw,
    conv_chip,
    wc_all,
    wa_all,
    part_out,
    part_in,
    attn_all,
    total_ref,
    stats,
    x_sem,
    turn_sem,
    w_sem,
    send_q,
    send_kv,
    recv_q,
    recv_kv,
    send_fwd,
    recv_fwd,
    send_o,
    recv_o,
    small_send,
    small_recv,
    send_wa,
    recv_wa,
    send_wf,
    send_wc,
    recv_wc,
    local_wc,
    send_part,
    recv_part,
    send_y,
    recv_y,
    send_s,
    recv_s,
    send_stat,
    recv_stat,
):
    j, t = lax.axis_index("sp"), lax.axis_index("tp")
    c, y = t % 2, t // 2
    ranks = tp // 2
    tok, model = x_ref.shape
    width = model // tp
    heads = q_own.shape[0]
    channels = wc_all.shape[2]
    half = n // 2
    repeat = half // heads
    parts = 2 * repeat
    rows = tok // parts
    per = TILE // VD
    pairs, tiles = heads // per, channels // TILE

    def remote(src, dst, send_sem, recv_sem, device):
        return pltpu.make_async_remote_copy(
            src_ref=src,
            dst_ref=dst,
            send_sem=send_sem,
            recv_sem=recv_sem,
            device_id=device,
            device_id_type=MESH,
        )

    sibling = (j, y * 2 + 1 - c)

    def peer(step):
        return (j, (y + step) % ranks * 2 + c)

    barrier = pltpu.get_barrier_semaphore()
    x_copy = pltpu.make_async_copy(x_hbm, x_ref, x_sem)
    x_copy.start()

    turn_copy = pltpu.make_async_copy(turn_ref, tables, turn_sem)
    turn_copy.start()
    products = 3 * (pairs + tiles)
    side = j // half
    early = c == side
    shift = jnp.where(jnp.logical_and(side == 1, c == 0), 0, 1)
    lead = jnp.where(early, 0, 3 * ((tiles + 1) // 2))

    def product(i):
        is_conv = jnp.logical_or(i < lead, i >= lead + 3 * pairs)
        r = jnp.where(i < lead, i, i - 3 * pairs)
        q = i - lead
        kind = jnp.where(is_conv, 3 + r % 3, (q // pairs + shift) % 3)
        index = jnp.where(is_conv, r // 3, (q % pairs + j) % pairs)
        return kind, index

    def load(i):
        kind, index = product(i)
        for w, ref in enumerate((wq_ref, wk_ref, wv_ref, wb_ref, wc_ref, wh_ref)):

            @pl.when(kind == w)
            def _():
                pltpu.make_async_copy(
                    ref.at[:, pl.ds(pl.multiple_of(index * TILE, TILE), TILE)],
                    wbuf.at[i % RING],
                    w_sem.at[i % RING],
                ).start()

    load(0)

    @pl.loop(0, n)
    def _(a):
        for e in range(2):

            @pl.when(jnp.logical_or(a != j, c != e))
            def _():
                pl.semaphore_signal(
                    barrier, inc=1, device_id=(a, y * 2 + e), device_id_type=MESH
                )

    @pl.loop(1, ranks)
    def _(step):
        for e in range(2):
            pl.semaphore_signal(
                barrier,
                inc=1,
                device_id=(j, (y + step) % ranks * 2 + e),
                device_id_type=MESH,
            )

    lane_row = lax.broadcasted_iota(jnp.int32, (1, VD), 1)
    cos_far, sin_far = base_ref[0, pl.ds(j, 1)], base_ref[1, pl.ds(j, 1)]
    turn_copy.wait()
    cos_ref[...] = cos_far * tables[0] - sin_far * tables[1]
    sin_ref[...] = jnp.where(lane_row % QK < QK // 2, -1.0, 1.0) * (
        sin_far * tables[0] + cos_far * tables[1]
    )
    for i in range(1, RING - 1):
        load(i)
    for h in range(heads):
        lam_all[c, h : h + 1] = jnp.full((1, VD), lam_ref[h], F32)

    rim_copy = remote(
        x_ref.at[pl.ds(tok - RIM, RIM)],
        rim_x,
        small_send.at[1],
        small_recv.at[1],
        (jnp.minimum(j + 1, n - 1), t),
    )
    lam_copy = remote(lam_all.at[c], lam_all.at[c], small_send.at[0], small_recv.at[0], sibling)

    def wa_rows(head, source):
        return wa_all.at[pl.ds(pl.multiple_of((head * tp + source) * VD, VD), VD)]

    def wa_block(head, target):
        return w_attn_ref.at[
            pl.ds(pl.multiple_of(head * VD, VD), VD),
            pl.ds(pl.multiple_of(target * width, VD), width),
        ]

    def wc_cols(rank, core):
        return w_conv_ref.at[:, pl.ds(pl.multiple_of((rank * 2 + core) * width, VD), width)]

    near = heads // 2
    first_near = (j % 2) * near

    def local_weights():
        for head in range(heads):
            pltpu.make_async_copy(
                wa_block(head, t), wa_rows(head, t), recv_wa.at[t, head]
            ).start()

        @pl.loop(0, ranks)
        def _(rank):
            pltpu.make_async_copy(wc_cols(rank, c), wc_all.at[rank, c], local_wc.at[rank]).start()

    def early_sends():
        pl.semaphore_wait(barrier, 2 * n - 1 + 2 * (ranks - 1))

        @pl.when(j + 1 < n)
        def _():
            rim_copy.start()

        lam_copy.start()

        @pl.loop(1, ranks)
        def _(step):
            for e in range(2):
                target = (y + step) % ranks * 2 + e
                for h in range(near):
                    head = first_near + h
                    remote(
                        wa_block(head, target),
                        wa_rows(head, t),
                        send_wa.at[target, head],
                        recv_wa.at[t, head],
                        (j, target),
                    ).start()

    def sibling_weights():
        for head in range(heads):
            target = y * 2 + 1 - c
            remote(
                wa_block(head, target),
                wa_rows(head, t),
                send_wa.at[target, head],
                recv_wa.at[t, head],
                sibling,
            ).start()

        @pl.loop(0, ranks)
        def _(rank):
            remote(
                wc_cols(rank, 1 - c),
                wc_all.at[rank, c],
                send_wc.at[rank],
                recv_wc.at[rank],
                sibling,
            ).start()

    def pass_weights():
        @pl.loop(1, ranks)
        def _(step):
            for e in range(2):
                source = (y + step) % ranks * 2 + e
                for h in range(near):
                    head = first_near + h
                    block = wa_rows(head, source)
                    arrived(block, recv_wa.at[source, head])
                    remote(
                        block,
                        block,
                        send_wf.at[source, h],
                        recv_wa.at[source, head],
                        (j + 1 - 2 * (j % 2), t),
                    ).start()

    def part_of(block, rep, core):
        part = rep * 2 + core
        return jnp.where(block % 2 == 0, part, parts - 1 - part)

    def put(src, dst, send_sem, recv_sem, device, here):
        @pl.when(here)
        def _():
            pltpu.make_async_copy(src, dst, recv_sem).start()

        @pl.when(jnp.logical_not(here))
        def _():
            remote(src, dst, send_sem, recv_sem, device).start()

    def sent(src, send_sem):
        remote(src, src, send_sem, send_sem, sibling).wait_send()

    def put_done(src, send_sem, here):
        @pl.when(jnp.logical_not(here))
        def _():
            sent(src, send_sem)

    def arrived(dst, recv_sem):
        pltpu.make_async_copy(dst, dst, recv_sem).wait()

    lane = lax.broadcasted_iota(jnp.int32, (tok, VD), 1)
    low = lane % QK < QK // 2
    fold = QK ** (-0.5) * math.log2(math.e)

    def rotate(values):
        values = values.astype(F32)
        partner = jnp.where(
            low, pltpu.roll(values, VD - QK // 2, 1), pltpu.roll(values, QK // 2, 1)
        )
        return values * cos_ref[...] + partner * sin_ref[...]

    def send_kv_of(e, pair):
        for p in range(per):
            head = pair * per + p
            for r in range(repeat):
                local = head * repeat + r
                s = c * half + local
                put(
                    kv_own.at[e, head],
                    kv_all.at[e, j],
                    send_kv.at[local * 2 + e],
                    recv_kv.at[j],
                    (s, y * 2 + e),
                    jnp.logical_and(s == j, c == e),
                )

    def send_q_of(pair):
        for p in range(per):
            head = pair * per + p
            for r in range(repeat):
                local = head * repeat + r
                s = c * half + local
                for e in range(2):
                    first = pl.multiple_of(part_of(j, r, e) * rows, 16)
                    put(
                        q_own.at[head, pl.ds(first, rows)],
                        q_all.at[j],
                        send_q.at[local * 2 + e],
                        recv_q.at[j],
                        (s, y * 2 + e),
                        jnp.logical_and(s == j, c == e),
                    )

    def convolve(g):
        cols = pl.ds(pl.multiple_of(g * TILE, TILE), TILE)
        gated = raw_ref[1].astype(F32) * raw_ref[2].astype(F32)
        before = jnp.where(j > 0, rim_raw[0] * rim_raw[1], 0.0)
        one, two = before[RIM - 1 :], before[RIM - 2 : RIM - 1]
        row = lax.broadcasted_iota(jnp.int32, gated.shape, 0)
        back_one = jnp.where(row == 0, one, pltpu.roll(gated, 1, 0))
        back_two = jnp.where(row == 0, two, jnp.where(row == 1, one, pltpu.roll(gated, 2, 0)))
        tap = taps_ref[:, cols].astype(F32)
        conv = tap[0:1] * back_two + tap[1:2] * back_one + tap[2:3] * gated
        conv_chip[c, :, cols] = (raw_ref[0].astype(F32) * conv).astype(BF16)


    def forward(block):
        here = kv_all.at[c, block]
        arrived(here, recv_kv.at[block])
        remote(here, here, send_fwd.at[block], recv_fwd.at[block], sibling).start()

    def keys_sent(first):
        @pl.loop(0, half)
        def _(b):
            forward(first + b)

    conv_copy = remote(
        conv_chip.at[c], conv_chip.at[c], small_send.at[2], small_recv.at[2], sibling
    )

    def conv_product(first, rank):
        span = pl.ds(first, SPAN)
        return jnp.dot(
            conv_chip[0, span], wc_all[rank, 0], preferred_element_type=F32
        ) + jnp.dot(conv_chip[1, span], wc_all[rank, 1], preferred_element_type=F32)

    def conv_parts():
        conv_copy.wait_recv()

        @pl.loop(0, ranks)
        def _(rank):
            mine = wc_all.at[rank, c]
            theirs = wc_all.at[rank, 1 - c]
            arrived(mine, local_wc.at[rank])
            arrived(theirs, recv_wc.at[rank])

        @pl.loop(1, ranks)
        def _(step):
            @pl.loop(0, tok // SPAN)
            def _(b):
                first = pl.multiple_of(b * SPAN, SPAN)
                span = pl.ds(first, SPAN)
                part_out[step - 1, span] = conv_product(first, (y + step) % ranks).astype(BF16)
                remote(
                    part_out.at[step - 1, span],
                    part_in.at[step - 1, span],
                    send_part.at[step - 1, b],
                    recv_part.at[step - 1, b],
                    peer(step),
                ).start()

    x_copy.wait()

    @pl.loop(0, products)
    def _(i):
        kind, index = product(i)

        @pl.when(i + RING - 1 < products)
        def _():
            load(i + RING - 1)

        arrived(wbuf.at[i % RING], w_sem.at[i % RING])
        raw_ref[kind % 3] = jnp.dot(
            x_ref[...], wbuf[i % RING], preferred_element_type=F32
        ).astype(BF16)

        @pl.when(i == 0)
        def _():
            early_sends()

        @pl.when(jnp.logical_and(kind >= 4, j > 0))
        def _():
            @pl.when(jnp.logical_and(kind == 4, index == 0))
            def _():
                rim_copy.wait_recv()

            rim_raw[kind - 4] = (
                jnp.dot(rim_x[...], wbuf[i % RING], preferred_element_type=F32)
                .astype(BF16)
                .astype(F32)
            )

        @pl.when(i == 2)
        def _():
            local_weights()
            sibling_weights()

        @pl.when(kind == 1)
        def _():
            for p in range(per):
                kv_own[0, index * per + p] = rotate(
                    raw_ref[1, :, p * VD : (p + 1) * VD]
                ).astype(BF16)
            send_kv_of(0, index)

        @pl.when(kind == 2)
        def _():
            for p in range(per):
                kv_own[1, index * per + p] = raw_ref[2, :, p * VD : (p + 1) * VD]
            send_kv_of(1, index)

        @pl.when(kind == 0)
        def _():
            for p in range(per):
                q_own[index * per + p] = (
                    rotate(raw_ref[0, :, p * VD : (p + 1) * VD]) * fold
                ).astype(BF16)
            send_q_of(index)

        @pl.when(kind == 5)
        def _():
            convolve(index)

    lam_copy.wait()
    conv_copy.start()
    keys_sent(side * half)
    conv_parts()
    pass_weights()

    head_at = (j % half) // repeat
    rep_at = j % repeat
    owner_tp = y * 2 + side
    lam = lam_all[side, pl.ds(head_at, 1)]
    gain = gain_ref[...].astype(F32)
    block_lane = lax.broadcasted_iota(jnp.int32, (rows, VD), 1)

    def attend(slot, kb, both, part, masked):
        k, v = kv_all[0, kb], kv_all[1, kb]
        s = lax.dot_general(both, k, (((1,), (1,)), ((), ())), preferred_element_type=F32)
        if masked:
            r = part * rows + lax.broadcasted_iota(jnp.int32, s.shape, 0) % rows
            s = jnp.where(lax.broadcasted_iota(jnp.int32, s.shape, 1) <= r, s, NEG_LARGE)
        slabs = [s[:, b * VD : (b + 1) * VD] for b in range(tok // VD)]
        old = m_ref[slot]
        top = functools.reduce(jnp.maximum, slabs)
        new = jnp.maximum(old, jnp.max(top, axis=1, keepdims=True))
        factor = jnp.exp2(old - new)
        total = l_ref[slot] * factor
        weights = []
        for slab in slabs:
            w = jnp.exp2(slab - new)
            total = total + w
            weights.append(w.astype(BF16))
        m_ref[slot] = new
        l_ref[slot] = total
        acc_ref[slot] = acc_ref[slot] * factor + jnp.dot(
            jnp.concatenate(weights, axis=1), v, preferred_element_type=F32
        )

    def piece(head, source, part):
        return attn_all.at[
            pl.ds(pl.multiple_of(part * rows, 16), rows),
            pl.ds(pl.multiple_of((head * tp + source) * VD, VD), VD),
        ]

    def piece_of(k, core, source):
        local = (j - k) % half
        head, rep = local // repeat, local % repeat
        return local * 2 + core, piece(head, source, part_of(j, rep, core))

    def share(k):
        for core in range(2):
            index, mine = piece_of(k, core, t)
            arrived(mine, recv_o.at[index])

            @pl.loop(1, ranks)
            def _(step):
                remote(
                    mine, mine, send_y.at[step, index], recv_y.at[step, index], peer(step)
                ).start()

            remote(mine, mine, send_s.at[y, index], recv_s.at[y, index], sibling).start()

    def relay(k):
        @pl.loop(1, ranks)
        def _(step):
            rank = (y + ranks - step) % ranks
            for core in range(2):
                index, theirs = piece_of(k, core, rank * 2 + c)
                arrived(theirs, recv_y.at[step, index])
                remote(
                    theirs, theirs, send_s.at[rank, index], recv_s.at[rank, index], sibling
                ).start()

    def gathered(k):
        @pl.loop(0, ranks)
        def _(rank):
            for core in range(2):
                index, theirs = piece_of(k, core, rank * 2 + 1 - c)
                arrived(theirs, recv_s.at[rank, index])

    @pl.loop(0, 3 * half)
    def _(step):
        phase = step // half
        turn = (step + j) % half
        group = jnp.where(phase == 0, side, jnp.where(phase == 1, 1, 1 - side))
        block = group * half + turn
        base = group * half
        slot = jnp.where(group == 0, half, turn)
        enter = step % half == 0
        other = (1 - side) * half

        def keys_ready(first):
            @pl.loop(0, half)
            def _(b):
                arrived(kv_all.at[1 - c, first + b], recv_fwd.at[first + b])

        def queries_ready(first):
            @pl.loop(0, half)
            def _(b):
                arrived(q_all.at[first + b], recv_q.at[first + b])

        @pl.when(jnp.logical_and(enter, phase == 0))
        def _():
            keys_ready(base)
            queries_ready(base)

        @pl.when(jnp.logical_and(enter, phase == 1 + side))
        def _():
            queries_ready(other)

        @pl.when(jnp.logical_and(enter, phase == 2 - side))
        def _():
            keys_sent(other)
            keys_ready(other)

        @pl.when(jnp.logical_and(early, step == 2 * half))
        def _():
            @pl.loop(0, half)
            def _(k):
                share(k)

        @pl.when(jnp.logical_and(early, step == 2 * half + 2))
        def _():
            @pl.loop(0, half)
            def _(k):
                relay(k)

        @pl.when(jnp.logical_and(jnp.logical_not(early), step > 2 * half + 1))
        def _():
            share(step - 2 * half - 2)

        q = q_all[block]
        zero = jnp.zeros_like(q)
        both = jnp.concatenate(
            [jnp.where(block_lane < QK, q, zero), jnp.where(block_lane < QK, zero, q)], axis=0
        )
        part = part_of(block, rep_at, c)

        @pl.when(phase == jnp.where(group == 0, phase, 1 - side))
        def _():
            m_ref[slot] = jnp.full(m_ref.shape[1:], NEG_LARGE, F32)
            l_ref[slot] = jnp.zeros(l_ref.shape[1:], F32)
            acc_ref[slot] = jnp.zeros(acc_ref.shape[1:], F32)

        @pl.loop(jnp.where(phase == 1, 0, base), jnp.where(phase == 1, half, block))
        def _(kb):
            attend(slot, kb, both, part, False)

        @pl.when(phase != 1)
        def _():
            attend(slot, block, both, part, True)

        @pl.when(phase >= jnp.where(group == 0, 0, 2 - side))
        def _():
            first, second = (
                acc_ref[slot, span] / jnp.sum(l_ref[slot, span], axis=1, keepdims=True)
                for span in (pl.ds(0, rows), pl.ds(rows, rows))
            )
            diff = first - lam * second
            norm = lax.rsqrt(jnp.mean(diff * diff, axis=1, keepdims=True) + 1e-05)
            out_own[block] = (diff * norm * gain).astype(BF16)
            put(
                out_own.at[block],
                piece(head_at, owner_tp, part),
                send_o.at[block],
                recv_o.at[(j % half) * 2 + c],
                (block, owner_tp),
                jnp.logical_and(block == j, side == c),
            )

    @pl.when(jnp.logical_not(early))
    def _():
        @pl.loop(half - 2, half)
        def _(k):
            share(k)

        @pl.loop(0, half - 1)
        def _(k):
            relay(k)

    @pl.loop(1, ranks)
    def _(step):
        @pl.loop(0, tok // SPAN)
        def _(b):
            arrived(part_in.at[step - 1, pl.ds(0, SPAN)], recv_part.at[step - 1, b])

    @pl.loop(0, tok // SPAN)
    def _(b):
        first = pl.multiple_of(b * SPAN, SPAN)
        value = conv_product(first, y)
        for step in range(1, ranks):
            value = value + part_in[step - 1, pl.ds(first, SPAN)].astype(F32)
        total_ref[pl.ds(first, SPAN)] = value

    for head in range(heads):
        for e in range(2):
            source = y * 2 + e
            arrived(wa_rows(head, source), recv_wa.at[source, head])

    @pl.loop(1, ranks)
    def _(step):
        for e in range(2):
            source = (y + step) % ranks * 2 + e
            for h in range(near):
                head = near - first_near + h
                arrived(wa_rows(head, source), recv_wa.at[source, head])

    def accumulate(k):
        gathered(k)
        local = (j - k) % half
        head, rep = local // repeat, local % repeat
        deep = pl.ds(pl.multiple_of(head * tp * VD, VD), tp * VD)
        for core in range(2):
            span = pl.ds(pl.multiple_of(part_of(j, rep, core) * rows, 16), rows)
            total_ref[span] = total_ref[span] + jnp.dot(
                attn_all[span, deep], wa_all[deep], preferred_element_type=F32
            )

    @pl.loop(0, half)
    def _(k):
        @pl.when(jnp.logical_and(jnp.logical_not(early), k == half - 1))
        def _():
            relay(half - 1)

        accumulate(k)

    slabs = width // VD

    @pl.loop(0, tok // SPAN)
    def _(b):
        span = pl.ds(pl.multiple_of(b * SPAN, SPAN), SPAN)
        mix = total_ref[span].astype(BF16)
        out_ref[span] = mix
        sums = jnp.zeros((SPAN, VD), F32)
        squares = jnp.zeros((SPAN, VD), F32)
        for s in range(slabs):
            slab = mix[:, s * VD : (s + 1) * VD].astype(F32)
            sums = sums + slab
            squares = squares + slab * slab
        stats[t, 0:1, span] = jnp.sum(sums.T, axis=0, keepdims=True)
        stats[t, 1:2, span] = jnp.sum(squares.T, axis=0, keepdims=True)

    def stat_copy(step):
        return remote(
            stats.at[t],
            stats.at[t],
            send_stat.at[step],
            recv_stat.at[step],
            (j, (t + step) % tp),
        )

    @pl.loop(1, tp)
    def _(step):
        stat_copy(step).start()

    @pl.loop(1, tp)
    def _(step):
        source = (t + tp - step) % tp
        arrived(stats.at[source], recv_stat.at[step])

    @pl.loop(0, tok // SPAN)
    def _(b):
        span = pl.ds(pl.multiple_of(b * SPAN, SPAN), SPAN)
        sums, squares = stats[0, 0:1, span], stats[0, 1:2, span]
        for source in range(1, tp):
            sums = sums + stats[source, 0:1, span]
            squares = squares + stats[source, 1:2, span]
        mean = sums / model
        scale = lax.rsqrt(squares / model - mean * mean + 1e-05)
        stat_ref[0:1, span] = mean
        stat_ref[1:2, span] = scale


    @pl.when(j + 1 < n)
    def _():
        rim_copy.wait_send()

    conv_copy.wait_send()

    @pl.loop(0, half)
    def _(local):
        head = local // repeat
        s = c * half + local
        for e in range(2):
            here = jnp.logical_and(s == j, c == e)
            put_done(kv_own.at[e, head], send_kv.at[local * 2 + e], here)
            put_done(q_own.at[head, pl.ds(0, rows)], send_q.at[local * 2 + e], here)

    @pl.loop(0, n)
    def _(block):
        sent(kv_all.at[c, block], send_fwd.at[block])
        put_done(out_own.at[block], send_o.at[block], jnp.logical_and(block == j, side == c))

        @pl.loop(1, ranks)
        def _(step):
            sent(out_own.at[0], send_y.at[step, block])

        @pl.loop(0, ranks)
        def _(rank):
            sent(out_own.at[0], send_s.at[rank, block])

    @pl.loop(1, tp)
    def _(step):
        stat_copy(step).wait_send()

    for head in range(heads):
        sent(wa_rows(head, t), send_wa.at[y * 2 + 1 - c, head])

    @pl.loop(1, ranks)
    def _(step):
        for e in range(2):
            other = (y + step) % ranks * 2 + e
            for h in range(near):
                sent(wa_rows(h, t), send_wa.at[other, first_near + h])
                sent(wa_rows(h, t), send_wf.at[other, h])

    @pl.loop(0, ranks)
    def _(rank):
        sent(wc_all.at[rank, c], send_wc.at[rank])

    @pl.loop(1, ranks)
    def _(step):
        @pl.loop(0, tok // SPAN)
        def _(b):
            sent(part_out.at[step - 1, pl.ds(0, SPAN)], send_part.at[step - 1, b])


def scale_kernel(mix_ref, stat_ref, gain_ref, out_ref):
    rows, width = mix_ref.shape
    mean = jnp.broadcast_to(stat_ref[0:1], (VD, rows)).T
    scale = jnp.broadcast_to(stat_ref[1:2], (VD, rows)).T
    for s in range(width // VD):
        cols = slice(s * VD, (s + 1) * VD)
        value = (mix_ref[:, cols].astype(F32) - mean) * scale
        out_ref[:, cols] = (value * gain_ref[:, cols]).astype(BF16)


def per_device(
    n,
    tp,
    hidden_states,
    w_conv_b,
    w_conv_c,
    w_conv_h,
    conv_taps,
    w_query,
    w_key,
    w_value,
    lambdas,
    head_gain,
    w_out_conv,
    w_out_attn,
    out_gain,
):
    tok, model = hidden_states.shape
    heads = w_value.shape[1] // VD
    channels = w_conv_b.shape[1]
    half = n // 2
    repeat = half // heads
    parts = 2 * repeat
    rows = tok // parts
    ranks = tp // 2
    width = model // tp

    inverse = 10000.0 ** (-np.arange(0, QK, 2, dtype=np.float64) / QK)
    inverse = np.tile(inverse, VD // inverse.size)[None, :]
    table = lambda angles: np.stack([np.cos(angles), np.sin(angles)]).astype(np.float32)
    turn = table(np.arange(tok)[:, None] * inverse)
    base = table(np.arange(n)[:, None] * tok * inverse)
    lam_rows = -(-heads // 8) * 8

    vmem, hbm = pl.BlockSpec(memory_space=pltpu.VMEM), pl.BlockSpec(memory_space=pl.ANY)
    smem = pl.BlockSpec(memory_space=pltpu.SMEM)
    dma = pltpu.SemaphoreType.DMA
    mix, stat = pl.pallas_call(
        functools.partial(mixer_kernel, n, tp),
        out_shape=(
            jax.ShapeDtypeStruct((tok, width), BF16),
            jax.ShapeDtypeStruct((8, tok), F32),
        ),
        in_specs=[hbm] + [vmem] * 2 + [smem] + [vmem] + [hbm] * 9,
        out_specs=(vmem, vmem),
        scratch_shapes=[
            pltpu.VMEM((tok, model), BF16),
            pltpu.VMEM((tok, VD), F32),
            pltpu.VMEM((tok, VD), F32),
            pltpu.VMEM((2, tok, VD), F32),
            pltpu.VMEM((RING, model, TILE), BF16),
            pltpu.VMEM((3, tok, TILE), BF16),
            pltpu.VMEM((heads, tok, VD), BF16),
            pltpu.VMEM((2, heads, tok, VD), BF16),
            pltpu.VMEM((n, rows, VD), BF16),
            pltpu.VMEM((2, n, tok, VD), BF16),
            pltpu.VMEM((n, rows, VD), BF16),
            pltpu.VMEM((half + 1, 2 * rows, VD), F32),
            pltpu.VMEM((half + 1, 2 * rows, VD), F32),
            pltpu.VMEM((half + 1, 2 * rows, VD), F32),
            pltpu.VMEM((2, lam_rows, VD), F32),
            pltpu.VMEM((RIM, model), BF16),
            pltpu.VMEM((2, RIM, TILE), F32),
            pltpu.VMEM((2, tok, channels), BF16),
            pltpu.VMEM((ranks, 2, channels, width), BF16),
            pltpu.VMEM((heads * tp * VD, width), BF16),
            pltpu.VMEM((max(ranks - 1, 1), tok, width), BF16),
            pltpu.VMEM((max(ranks - 1, 1), tok, width), BF16),
            pltpu.VMEM((tok, heads * tp * VD), BF16),
            pltpu.VMEM((tok, width), F32),
            pltpu.VMEM((tp, 8, tok), F32),
            dma,
            dma,
            dma((RING,)),
            dma((n,)),
            dma((n,)),
            dma((n,)),
            dma((n,)),
            dma((n,)),
            dma((n,)),
            dma((n,)),
            dma((n,)),
            dma((3,)),
            dma((3,)),
            dma((tp, heads)),
            dma((tp, heads)),
            dma((tp, heads)),
            dma((ranks,)),
            dma((ranks,)),
            dma((ranks,)),
            dma((ranks, tok // SPAN)),
            dma((ranks, tok // SPAN)),
            dma((ranks, n)),
            dma((ranks, n)),
            dma((ranks, n)),
            dma((ranks, n)),
            dma((tp,)),
            dma((tp,)),
        ],
        compiler_params=pltpu.CompilerParams(
            vmem_limit_bytes=VMEM_LIMIT, collective_id=0, has_side_effects=True
        ),
        cost_estimate=pl.CostEstimate(
            flops=12 * tok * model * channels + 4 * n * n * rows * tok * VD,
            bytes_accessed=2 * model * (tok + 6 * channels),
            transcendentals=0,
        ),
        name="mixer",
    )(
        jnp.asarray(turn),
        jnp.asarray(base),
        conv_taps,
        lambdas,
        head_gain[None],
        hidden_states,
        w_query,
        w_key,
        w_value,
        w_conv_b,
        w_conv_c,
        w_conv_h,
        w_out_conv,
        w_out_attn,
    )
    own_gain = lax.dynamic_slice_in_dim(out_gain, lax.axis_index("tp") * width, width, 0)
    grid = tok // SPAN
    return pl.pallas_call(
        scale_kernel,
        grid=(grid,),
        out_shape=jax.ShapeDtypeStruct((tok, width), BF16),
        in_specs=[
            pl.BlockSpec((SPAN, width), lambda i: (i, 0)),
            pl.BlockSpec((8, SPAN), lambda i: (0, i)),
            pl.BlockSpec((1, width), lambda i: (0, 0)),
        ],
        out_specs=pl.BlockSpec((SPAN, width), lambda i: (i, 0)),
        cost_estimate=pl.CostEstimate(
            flops=4 * tok * width, bytes_accessed=4 * tok * width, transcendentals=0
        ),
        name="scale",
    )(mix, stat, own_gain.astype(F32)[None, :])


def solution(mesh):
    n, tp = mesh.shape["sp"], mesh.shape["tp"]
    return jax.shard_map(
        functools.partial(per_device, n, tp),
        mesh=mesh,
        in_specs=(
            P("sp", None),
            P(None, "tp"),
            P(None, "tp"),
            P(None, "tp"),
            P(None, "tp"),
            P(None, "tp"),
            P(None, "tp"),
            P(None, "tp"),
            P("tp"),
            P(),
            P("tp", None),
            P("tp", None),
            P(),
        ),
        out_specs=P("sp", "tp"),
        check_vma=False,
    )
```

```python
import functools
import math

import jax
import jax.numpy as jnp
import numpy as np
from jax import lax
from jax.experimental import pallas as pl
from jax.experimental.pallas import tpu as pltpu
from jax.sharding import PartitionSpec as P

QK = 64
VD = 128
TILE = 256
SPAN = 256
RIM = 16
RING = 4
NEG_LARGE = -1e30
VMEM_LIMIT = 67_000_000
MESH = pl.DeviceIdType.MESH
BF16, F32 = jnp.bfloat16, jnp.float32


def mixer_kernel(
    n,
    tp,
    turn_ref,
    base_ref,
    taps_ref,
    lam_ref,
    gain_ref,
    x_hbm,
    wq_ref,
    wk_ref,
    wv_ref,
    wb_ref,
    wc_ref,
    wh_ref,
    w_conv_ref,
    w_attn_ref,
    out_ref,
    stat_ref,
    x_ref,
    cos_ref,
    sin_ref,
    tables,
    wbuf,
    raw_ref,
    q_own,
    kv_own,
    q_all,
    kv_all,
    out_own,
    m_ref,
    l_ref,
    acc_ref,
    lam_all,
    rim_x,
    rim_raw,
    conv_chip,
    wc_all,
    wa_all,
    part_out,
    part_in,
    attn_all,
    total_ref,
    mix_ref,
    stats,
    x_sem,
    turn_sem,
    w_sem,
    send_q,
    send_kv,
    recv_q,
    recv_kv,
    send_fwd,
    recv_fwd,
    send_o,
    recv_o,
    small_send,
    small_recv,
    send_wa,
    recv_wa,
    send_wf,
    send_wc,
    recv_wc,
    local_wc,
    send_part,
    recv_part,
    send_y,
    recv_y,
    send_s,
    recv_s,
    send_stat,
    recv_stat,
    mix_sem,
):
    j, t = lax.axis_index("sp"), lax.axis_index("tp")
    c, y = t % 2, t // 2
    ranks = tp // 2
    tok, model = x_ref.shape
    width = model // tp
    heads = q_own.shape[0]
    channels = wc_all.shape[2]
    half = n // 2
    repeat = half // heads
    parts = 2 * repeat
    rows = tok // parts
    per = TILE // VD
    pairs, tiles = heads // per, channels // TILE

    def remote(src, dst, send_sem, recv_sem, device):
        return pltpu.make_async_remote_copy(
            src_ref=src,
            dst_ref=dst,
            send_sem=send_sem,
            recv_sem=recv_sem,
            device_id=device,
            device_id_type=MESH,
        )

    sibling = (j, y * 2 + 1 - c)

    def peer(step):
        return (j, (y + step) % ranks * 2 + c)

    barrier = pltpu.get_barrier_semaphore()
    x_copy = pltpu.make_async_copy(x_hbm, x_ref, x_sem)
    x_copy.start()

    turn_copy = pltpu.make_async_copy(turn_ref, tables, turn_sem)
    turn_copy.start()
    products = 3 * (pairs + tiles)
    side = j // half
    early = c == side
    shift = jnp.where(jnp.logical_and(side == 1, c == 0), 0, 1)
    lead = jnp.where(early, 0, tiles)

    def product(i):
        is_conv = jnp.logical_or(i < lead, i >= lead + 3 * pairs)
        r = jnp.where(i < lead, i, i - 3 * pairs)
        q = i - lead
        gate = r < tiles
        conv_kind = jnp.where(gate, 3, 4 + (r - tiles) % 2)
        conv_index = jnp.where(gate, r, (r - tiles) // 2)
        kind = jnp.where(is_conv, conv_kind, (q // pairs + shift) % 3)
        index = jnp.where(is_conv, conv_index, (q % pairs + j) % pairs)
        return kind, index

    def load(i):
        kind, index = product(i)
        for w, ref in enumerate((wq_ref, wk_ref, wv_ref, wb_ref, wc_ref, wh_ref)):

            @pl.when(kind == w)
            def _():
                pltpu.make_async_copy(
                    ref.at[:, pl.ds(pl.multiple_of(index * TILE, TILE), TILE)],
                    wbuf.at[i % RING],
                    w_sem.at[i % RING],
                ).start()

    load(0)

    @pl.loop(0, n)
    def _(a):
        for e in range(2):

            @pl.when(jnp.logical_or(a != j, c != e))
            def _():
                pl.semaphore_signal(
                    barrier, inc=1, device_id=(a, y * 2 + e), device_id_type=MESH
                )

    @pl.loop(1, ranks)
    def _(step):
        for e in range(2):
            pl.semaphore_signal(
                barrier,
                inc=1,
                device_id=(j, (y + step) % ranks * 2 + e),
                device_id_type=MESH,
            )

    lane_row = lax.broadcasted_iota(jnp.int32, (1, VD), 1)
    cos_far, sin_far = base_ref[0, pl.ds(j, 1)], base_ref[1, pl.ds(j, 1)]
    turn_copy.wait()
    cos_ref[...] = cos_far * tables[0] - sin_far * tables[1]
    sin_ref[...] = jnp.where(lane_row % QK < QK // 2, -1.0, 1.0) * (
        sin_far * tables[0] + cos_far * tables[1]
    )
    for i in range(1, RING - 1):
        load(i)
    for h in range(heads):
        lam_all[c, h : h + 1] = jnp.full((1, VD), lam_ref[h], F32)

    rim_copy = remote(
        x_ref.at[pl.ds(tok - RIM, RIM)],
        rim_x,
        small_send.at[1],
        small_recv.at[1],
        (jnp.minimum(j + 1, n - 1), t),
    )
    lam_copy = remote(lam_all.at[c], lam_all.at[c], small_send.at[0], small_recv.at[0], sibling)

    def place(head, source):
        order = source % 2 * ranks + source // 2
        return pl.multiple_of((head * tp + order) * VD, VD)

    def wa_rows(head, source):
        return wa_all.at[pl.ds(place(head, source), VD)]

    def wa_block(head, target):
        return w_attn_ref.at[
            pl.ds(pl.multiple_of(head * VD, VD), VD),
            pl.ds(pl.multiple_of(target * width, VD), width),
        ]

    def wc_cols(rank, core):
        return w_conv_ref.at[:, pl.ds(pl.multiple_of((rank * 2 + core) * width, VD), width)]

    near = heads // 2
    first_near = (j % 2) * near

    def local_weights():
        for head in range(heads):
            pltpu.make_async_copy(
                wa_block(head, t), wa_rows(head, t), recv_wa.at[t, head]
            ).start()

        @pl.loop(0, ranks)
        def _(rank):
            pltpu.make_async_copy(wc_cols(rank, c), wc_all.at[rank, c], local_wc.at[rank]).start()

    def early_sends():
        pl.semaphore_wait(barrier, 2 * n - 1 + 2 * (ranks - 1))

        @pl.when(j + 1 < n)
        def _():
            rim_copy.start()

        lam_copy.start()

        @pl.loop(1, ranks)
        def _(step):
            for e in range(2):
                target = (y + step) % ranks * 2 + e
                for h in range(near):
                    head = first_near + h
                    remote(
                        wa_block(head, target),
                        wa_rows(head, t),
                        send_wa.at[target, head],
                        recv_wa.at[t, head],
                        (j, target),
                    ).start()

    def sibling_weights():
        for head in range(heads):
            target = y * 2 + 1 - c
            remote(
                wa_block(head, target),
                wa_rows(head, t),
                send_wa.at[target, head],
                recv_wa.at[t, head],
                sibling,
            ).start()

        @pl.loop(0, ranks)
        def _(rank):
            remote(
                wc_cols(rank, 1 - c),
                wc_all.at[rank, c],
                send_wc.at[rank],
                recv_wc.at[rank],
                sibling,
            ).start()

    def pass_weights():
        @pl.loop(1, ranks)
        def _(step):
            for e in range(2):
                source = (y + step) % ranks * 2 + e
                for h in range(near):
                    head = first_near + h
                    block = wa_rows(head, source)
                    arrived(block, recv_wa.at[source, head])
                    remote(
                        block,
                        block,
                        send_wf.at[source, h],
                        recv_wa.at[source, head],
                        (j + 1 - 2 * (j % 2), t),
                    ).start()

    def part_of(block, rep, core):
        part = rep * 2 + core
        return jnp.where(block % 2 == 0, part, parts - 1 - part)

    def put(src, dst, send_sem, recv_sem, device, here):
        @pl.when(here)
        def _():
            pltpu.make_async_copy(src, dst, recv_sem).start()

        @pl.when(jnp.logical_not(here))
        def _():
            remote(src, dst, send_sem, recv_sem, device).start()

    def sent(src, send_sem):
        remote(src, src, send_sem, send_sem, sibling).wait_send()

    def put_done(src, send_sem, here):
        @pl.when(jnp.logical_not(here))
        def _():
            sent(src, send_sem)

    def arrived(dst, recv_sem):
        pltpu.make_async_copy(dst, dst, recv_sem).wait()

    lane = lax.broadcasted_iota(jnp.int32, (tok, VD), 1)
    low = lane % QK < QK // 2
    fold = QK ** (-0.5) * math.log2(math.e)

    def rotate(values):
        values = values.astype(F32)
        partner = jnp.where(
            low, pltpu.roll(values, VD - QK // 2, 1), pltpu.roll(values, QK // 2, 1)
        )
        return values * cos_ref[...] + partner * sin_ref[...]

    def send_kv_of(e, pair):
        for p in range(per):
            head = pair * per + p
            for r in range(repeat):
                local = head * repeat + r
                s = c * half + local
                put(
                    kv_own.at[e, head],
                    kv_all.at[e, j],
                    send_kv.at[local * 2 + e],
                    recv_kv.at[j],
                    (s, y * 2 + e),
                    jnp.logical_and(s == j, c == e),
                )

    def send_q_of(pair):
        for p in range(per):
            head = pair * per + p
            for r in range(repeat):
                local = head * repeat + r
                s = c * half + local
                for e in range(2):
                    first = pl.multiple_of(part_of(j, r, e) * rows, 16)
                    put(
                        q_own.at[head, pl.ds(first, rows)],
                        q_all.at[j],
                        send_q.at[local * 2 + e],
                        recv_q.at[j],
                        (s, y * 2 + e),
                        jnp.logical_and(s == j, c == e),
                    )

    def convolve(g):
        cols = pl.ds(pl.multiple_of(g * TILE, TILE), TILE)
        gated = raw_ref[1].astype(F32) * raw_ref[2].astype(F32)
        before = jnp.where(j > 0, rim_raw[0] * rim_raw[1], 0.0)
        one, two = before[RIM - 1 :], before[RIM - 2 : RIM - 1]
        row = lax.broadcasted_iota(jnp.int32, gated.shape, 0)
        back_one = jnp.where(row == 0, one, pltpu.roll(gated, 1, 0))
        back_two = jnp.where(row == 0, two, jnp.where(row == 1, one, pltpu.roll(gated, 2, 0)))
        tap = taps_ref[:, cols].astype(F32)
        conv = tap[0:1] * back_two + tap[1:2] * back_one + tap[2:3] * gated
        conv_chip[c, :, cols] = (raw_ref[3 + g].astype(F32) * conv).astype(BF16)


    def forward(block):
        here = kv_all.at[c, block]
        arrived(here, recv_kv.at[block])
        remote(here, here, send_fwd.at[block], recv_fwd.at[block], sibling).start()

    def keys_sent(first):
        @pl.loop(0, half)
        def _(b):
            forward(first + b)

    conv_copy = remote(
        conv_chip.at[c], conv_chip.at[c], small_send.at[2], small_recv.at[2], sibling
    )

    def conv_product(first, rank):
        span = pl.ds(first, SPAN)
        return jnp.dot(
            conv_chip[0, span], wc_all[rank, 0], preferred_element_type=F32
        ) + jnp.dot(conv_chip[1, span], wc_all[rank, 1], preferred_element_type=F32)

    def conv_parts():
        conv_copy.wait_recv()

        @pl.loop(0, ranks)
        def _(rank):
            mine = wc_all.at[rank, c]
            theirs = wc_all.at[rank, 1 - c]
            arrived(mine, local_wc.at[rank])
            arrived(theirs, recv_wc.at[rank])

        @pl.loop(1, ranks)
        def _(step):
            @pl.loop(0, tok // SPAN)
            def _(b):
                first = pl.multiple_of(b * SPAN, SPAN)
                span = pl.ds(first, SPAN)
                part_out[step - 1, span] = conv_product(first, (y + step) % ranks).astype(BF16)
                remote(
                    part_out.at[step - 1, span],
                    part_in.at[step - 1, span],
                    send_part.at[step - 1, b],
                    recv_part.at[step - 1, b],
                    peer(step),
                ).start()

    x_copy.wait()

    @pl.loop(0, products)
    def _(i):
        kind, index = product(i)

        @pl.when(i + RING - 1 < products)
        def _():
            load(i + RING - 1)

        arrived(wbuf.at[i % RING], w_sem.at[i % RING])
        raw_ref[jnp.where(kind == 3, 3 + index, kind % 3)] = jnp.dot(
            x_ref[...], wbuf[i % RING], preferred_element_type=F32
        ).astype(BF16)

        @pl.when(i == 0)
        def _():
            early_sends()

        @pl.when(jnp.logical_and(kind >= 4, j > 0))
        def _():
            @pl.when(jnp.logical_and(kind == 4, index == 0))
            def _():
                rim_copy.wait_recv()

            rim_raw[kind - 4] = (
                jnp.dot(rim_x[...], wbuf[i % RING], preferred_element_type=F32)
                .astype(BF16)
                .astype(F32)
            )

        @pl.when(i == 2)
        def _():
            local_weights()
            sibling_weights()

        @pl.when(kind == 1)
        def _():
            for p in range(per):
                kv_own[0, index * per + p] = rotate(
                    raw_ref[1, :, p * VD : (p + 1) * VD]
                ).astype(BF16)
            send_kv_of(0, index)

        @pl.when(kind == 2)
        def _():
            for p in range(per):
                kv_own[1, index * per + p] = raw_ref[2, :, p * VD : (p + 1) * VD]
            send_kv_of(1, index)

        @pl.when(kind == 0)
        def _():
            for p in range(per):
                q_own[index * per + p] = (
                    rotate(raw_ref[0, :, p * VD : (p + 1) * VD]) * fold
                ).astype(BF16)
            send_q_of(index)

        @pl.when(kind == 5)
        def _():
            convolve(index)

    lam_copy.wait()
    conv_copy.start()
    keys_sent(side * half)
    conv_parts()
    pass_weights()

    head_at = (j % half) // repeat
    rep_at = j % repeat
    owner_tp = y * 2 + side
    lam = lam_all[side, pl.ds(head_at, 1)]
    gain = gain_ref[...].astype(F32)
    block_lane = lax.broadcasted_iota(jnp.int32, (rows, VD), 1)

    def scores(both, kb, part, masked):
        s = lax.dot_general(
            both, kv_all[0, kb], (((1,), (1,)), ((), ())), preferred_element_type=F32
        )
        if masked:
            r = part * rows + lax.broadcasted_iota(jnp.int32, s.shape, 0) % rows
            s = jnp.where(lax.broadcasted_iota(jnp.int32, s.shape, 1) <= r, s, NEG_LARGE)
        return s

    def attend(slot, both, part, jobs):
        ahead = scores(both, jobs[0][0], part, jobs[0][1])
        for number, (kb, _) in enumerate(jobs):
            s = ahead
            if number + 1 < len(jobs):
                ahead = scores(both, jobs[number + 1][0], part, jobs[number + 1][1])
            weigh(slot, s, kv_all[1, kb])

    def weigh(slot, s, v):
        slabs = [s[:, b * VD : (b + 1) * VD] for b in range(tok // VD)]
        old = m_ref[slot]
        top = functools.reduce(jnp.maximum, slabs)
        new = jnp.maximum(old, jnp.max(top, axis=1, keepdims=True))
        factor = jnp.exp2(old - new)
        total = l_ref[slot] * factor
        weights = []
        for slab in slabs:
            w = jnp.exp2(slab - new)
            total = total + w
            weights.append(w.astype(BF16))
        m_ref[slot] = new
        l_ref[slot] = total
        acc_ref[slot] = acc_ref[slot] * factor + jnp.dot(
            jnp.concatenate(weights, axis=1), v, preferred_element_type=F32
        )

    def piece(head, source, part):
        return attn_all.at[
            pl.ds(pl.multiple_of(part * rows, 16), rows),
            pl.ds(place(head, source), VD),
        ]

    def piece_of(k, core, source):
        local = (j - k) % half
        head, rep = local // repeat, local % repeat
        return local * 2 + core, piece(head, source, part_of(j, rep, core))

    def share(k):
        for core in range(2):
            index, mine = piece_of(k, core, t)
            arrived(mine, recv_o.at[index])

            @pl.loop(1, ranks)
            def _(step):
                remote(
                    mine, mine, send_y.at[step, index], recv_y.at[step, index], peer(step)
                ).start()

            remote(mine, mine, send_s.at[y, index], recv_s.at[y, index], sibling).start()

    def relay(k):
        @pl.loop(1, ranks)
        def _(step):
            rank = (y + ranks - step) % ranks
            for core in range(2):
                index, theirs = piece_of(k, core, rank * 2 + c)
                arrived(theirs, recv_y.at[step, index])
                remote(
                    theirs, theirs, send_s.at[rank, index], recv_s.at[rank, index], sibling
                ).start()

    def gathered(k):
        @pl.loop(0, ranks)
        def _(rank):
            for core in range(2):
                index, theirs = piece_of(k, core, rank * 2 + 1 - c)
                arrived(theirs, recv_s.at[rank, index])

    def own_product():
        @pl.loop(1, ranks)
        def _(step):
            @pl.loop(0, tok // SPAN)
            def _(b):
                arrived(part_in.at[step - 1, pl.ds(0, SPAN)], recv_part.at[step - 1, b])

        @pl.loop(0, tok // SPAN)
        def _(b):
            first = pl.multiple_of(b * SPAN, SPAN)
            value = conv_product(first, y)
            for step in range(1, ranks):
                value = value + part_in[step - 1, pl.ds(first, SPAN)].astype(F32)
            total_ref[pl.ds(first, SPAN)] = value

    @pl.loop(0, 3 * half)
    def _(step):
        phase = step // half
        turn = (step + j) % half
        group = jnp.where(phase == 0, side, jnp.where(phase == 1, 1, 1 - side))
        block = group * half + turn
        base = group * half
        slot = jnp.where(group == 0, half, turn)
        enter = step % half == 0
        other = (1 - side) * half

        def keys_ready(first):
            @pl.loop(0, half)
            def _(b):
                arrived(kv_all.at[1 - c, first + b], recv_fwd.at[first + b])

        def queries_ready(first):
            @pl.loop(0, half)
            def _(b):
                arrived(q_all.at[first + b], recv_q.at[first + b])

        @pl.when(jnp.logical_and(enter, phase == 0))
        def _():
            keys_ready(base)
            queries_ready(base)

        @pl.when(jnp.logical_and(enter, phase == 1 + side))
        def _():
            queries_ready(other)

        @pl.when(step == jnp.where(side == 0, 2 * half - 1, half))
        def _():
            keys_sent(other)

        @pl.when(jnp.logical_and(enter, phase == 2 - side))
        def _():
            keys_ready(other)

        @pl.when(step == 2 * half + 2)
        def _():
            own_product()

        @pl.when(jnp.logical_and(early, step == 2 * half))
        def _():
            @pl.loop(0, half)
            def _(k):
                share(k)

        @pl.when(jnp.logical_and(early, step == 2 * half + 2))
        def _():
            @pl.loop(0, half)
            def _(k):
                relay(k)

        @pl.when(jnp.logical_and(jnp.logical_not(early), step > 2 * half + 1))
        def _():
            share(step - 2 * half - 2)

        q = q_all[block]
        zero = jnp.zeros_like(q)
        both = jnp.concatenate(
            [jnp.where(block_lane < QK, q, zero), jnp.where(block_lane < QK, zero, q)], axis=0
        )
        part = part_of(block, rep_at, c)

        @pl.when(phase == jnp.where(group == 0, phase, 1 - side))
        def _():
            m_ref[slot] = jnp.full(m_ref.shape[1:], NEG_LARGE, F32)
            l_ref[slot] = jnp.zeros(l_ref.shape[1:], F32)
            acc_ref[slot] = jnp.zeros(acc_ref.shape[1:], F32)

        low_kb = jnp.where(phase == 1, 0, base)
        count = jnp.where(phase == 1, half, block - base)

        @pl.loop(0, count // 2)
        def _(p):
            kb = low_kb + 2 * p
            attend(slot, both, part, [(kb, False), (kb + 1, False)])

        @pl.when(jnp.logical_and(phase != 1, count % 2 == 1))
        def _():
            attend(slot, both, part, [(block - 1, False), (block, True)])

        @pl.when(jnp.logical_and(phase != 1, count % 2 == 0))
        def _():
            attend(slot, both, part, [(block, True)])

        @pl.when(phase >= jnp.where(group == 0, 0, 2 - side))
        def _():
            first, second = (
                acc_ref[slot, span] / jnp.sum(l_ref[slot, span], axis=1, keepdims=True)
                for span in (pl.ds(0, rows), pl.ds(rows, rows))
            )
            diff = first - lam * second
            norm = lax.rsqrt(jnp.mean(diff * diff, axis=1, keepdims=True) + 1e-05)
            out_own[block] = (diff * norm * gain).astype(BF16)
            put(
                out_own.at[block],
                piece(head_at, owner_tp, part),
                send_o.at[block],
                recv_o.at[(j % half) * 2 + c],
                (block, owner_tp),
                jnp.logical_and(block == j, side == c),
            )

    for head in range(heads):
        for e in range(2):
            source = y * 2 + e
            arrived(wa_rows(head, source), recv_wa.at[source, head])

    @pl.loop(1, ranks)
    def _(step):
        for e in range(2):
            source = (y + step) % ranks * 2 + e
            for h in range(near):
                head = near - first_near + h
                arrived(wa_rows(head, source), recv_wa.at[source, head])

    def accumulate(k, group):
        @pl.when(c != group)
        def _():
            gathered(k)

        local = (j - k) % half
        head, rep = local // repeat, local % repeat
        deep = pl.ds(place(head, group), ranks * VD)
        for core in range(2):
            span = pl.ds(pl.multiple_of(part_of(j, rep, core) * rows, 16), rows)
            total_ref[span] = total_ref[span] + jnp.dot(
                attn_all[span, deep], wa_all[deep], preferred_element_type=F32
            )

    @pl.loop(0, half)
    def _(k):
        accumulate(k, side)

    @pl.when(jnp.logical_not(early))
    def _():
        @pl.loop(half - 2, half)
        def _(k):
            share(k)

        @pl.loop(0, half)
        def _(k):
            relay(k)

    @pl.loop(0, half)
    def _(k):
        accumulate(k, 1 - side)

    slabs = width // VD

    def mix_copy(b):
        span = pl.ds(pl.multiple_of(b * SPAN, SPAN), SPAN)
        return pltpu.make_async_copy(mix_ref.at[span], out_ref.at[span], mix_sem.at[b])

    @pl.loop(0, tok // SPAN)
    def _(b):
        span = pl.ds(pl.multiple_of(b * SPAN, SPAN), SPAN)
        mix = total_ref[span].astype(BF16)
        mix_ref[span] = mix
        mix_copy(b).start()
        sums = jnp.zeros((SPAN, VD), F32)
        squares = jnp.zeros((SPAN, VD), F32)
        for s in range(slabs):
            slab = mix[:, s * VD : (s + 1) * VD].astype(F32)
            sums = sums + slab
            squares = squares + slab * slab
        stats[t, 0:1, span] = jnp.sum(sums.T, axis=0, keepdims=True)
        stats[t, 1:2, span] = jnp.sum(squares.T, axis=0, keepdims=True)

    def stat_copy(step):
        return remote(
            stats.at[t],
            stats.at[t],
            send_stat.at[step],
            recv_stat.at[step],
            (j, (t + step) % tp),
        )

    @pl.loop(1, tp)
    def _(step):
        stat_copy(step).start()

    @pl.loop(1, tp)
    def _(step):
        source = (t + tp - step) % tp
        arrived(stats.at[source], recv_stat.at[step])

    @pl.loop(0, tok // SPAN)
    def _(b):
        span = pl.ds(pl.multiple_of(b * SPAN, SPAN), SPAN)
        sums, squares = stats[0, 0:1, span], stats[0, 1:2, span]
        for source in range(1, tp):
            sums = sums + stats[source, 0:1, span]
            squares = squares + stats[source, 1:2, span]
        mean = sums / model
        scale = lax.rsqrt(squares / model - mean * mean + 1e-05)
        stat_ref[0:1, span] = mean
        stat_ref[1:2, span] = scale


    @pl.loop(0, tok // SPAN)
    def _(b):
        mix_copy(b).wait()

    @pl.when(j + 1 < n)
    def _():
        rim_copy.wait_send()

    conv_copy.wait_send()

    @pl.loop(0, half)
    def _(local):
        head = local // repeat
        s = c * half + local
        for e in range(2):
            here = jnp.logical_and(s == j, c == e)
            put_done(kv_own.at[e, head], send_kv.at[local * 2 + e], here)
            put_done(q_own.at[head, pl.ds(0, rows)], send_q.at[local * 2 + e], here)

    @pl.loop(0, n)
    def _(block):
        sent(kv_all.at[c, block], send_fwd.at[block])
        put_done(out_own.at[block], send_o.at[block], jnp.logical_and(block == j, side == c))

        @pl.loop(1, ranks)
        def _(step):
            sent(out_own.at[0], send_y.at[step, block])

        @pl.loop(0, ranks)
        def _(rank):
            sent(out_own.at[0], send_s.at[rank, block])

    @pl.loop(1, tp)
    def _(step):
        stat_copy(step).wait_send()

    for head in range(heads):
        sent(wa_rows(head, t), send_wa.at[y * 2 + 1 - c, head])

    @pl.loop(1, ranks)
    def _(step):
        for e in range(2):
            other = (y + step) % ranks * 2 + e
            for h in range(near):
                sent(wa_rows(h, t), send_wa.at[other, first_near + h])
                sent(wa_rows(h, t), send_wf.at[other, h])

    @pl.loop(0, ranks)
    def _(rank):
        sent(wc_all.at[rank, c], send_wc.at[rank])

    @pl.loop(1, ranks)
    def _(step):
        @pl.loop(0, tok // SPAN)
        def _(b):
            sent(part_out.at[step - 1, pl.ds(0, SPAN)], send_part.at[step - 1, b])


def scale_kernel(mix_ref, stat_ref, gain_ref, out_ref):
    rows, width = mix_ref.shape
    mean = jnp.broadcast_to(stat_ref[0:1], (VD, rows)).T
    scale = jnp.broadcast_to(stat_ref[1:2], (VD, rows)).T
    for s in range(width // VD):
        cols = slice(s * VD, (s + 1) * VD)
        value = (mix_ref[:, cols].astype(F32) - mean) * scale
        out_ref[:, cols] = (value * gain_ref[:, cols]).astype(BF16)


def per_device(
    n,
    tp,
    hidden_states,
    w_conv_b,
    w_conv_c,
    w_conv_h,
    conv_taps,
    w_query,
    w_key,
    w_value,
    lambdas,
    head_gain,
    w_out_conv,
    w_out_attn,
    out_gain,
):
    tok, model = hidden_states.shape
    heads = w_value.shape[1] // VD
    channels = w_conv_b.shape[1]
    half = n // 2
    repeat = half // heads
    parts = 2 * repeat
    rows = tok // parts
    ranks = tp // 2
    width = model // tp

    inverse = 10000.0 ** (-np.arange(0, QK, 2, dtype=np.float64) / QK)
    inverse = np.tile(inverse, VD // inverse.size)[None, :]
    table = lambda angles: np.stack([np.cos(angles), np.sin(angles)]).astype(np.float32)
    turn = table(np.arange(tok)[:, None] * inverse)
    base = table(np.arange(n)[:, None] * tok * inverse)
    lam_rows = -(-heads // 8) * 8

    vmem, hbm = pl.BlockSpec(memory_space=pltpu.VMEM), pl.BlockSpec(memory_space=pl.ANY)
    smem = pl.BlockSpec(memory_space=pltpu.SMEM)
    dma = pltpu.SemaphoreType.DMA
    mix, stat = pl.pallas_call(
        functools.partial(mixer_kernel, n, tp),
        out_shape=(
            jax.ShapeDtypeStruct((tok, width), BF16),
            jax.ShapeDtypeStruct((8, tok), F32),
        ),
        in_specs=[hbm] + [vmem] * 2 + [smem] + [vmem] + [hbm] * 9,
        out_specs=(hbm, vmem),
        scratch_shapes=[
            pltpu.VMEM((tok, model), BF16),
            pltpu.VMEM((tok, VD), F32),
            pltpu.VMEM((tok, VD), F32),
            pltpu.VMEM((2, tok, VD), F32),
            pltpu.VMEM((RING, model, TILE), BF16),
            pltpu.VMEM((3 + channels // TILE, tok, TILE), BF16),
            pltpu.VMEM((heads, tok, VD), BF16),
            pltpu.VMEM((2, heads, tok, VD), BF16),
            pltpu.VMEM((n, rows, VD), BF16),
            pltpu.VMEM((2, n, tok, VD), BF16),
            pltpu.VMEM((n, rows, VD), BF16),
            pltpu.VMEM((half + 1, 2 * rows, VD), F32),
            pltpu.VMEM((half + 1, 2 * rows, VD), F32),
            pltpu.VMEM((half + 1, 2 * rows, VD), F32),
            pltpu.VMEM((2, lam_rows, VD), F32),
            pltpu.VMEM((RIM, model), BF16),
            pltpu.VMEM((2, RIM, TILE), F32),
            pltpu.VMEM((2, tok, channels), BF16),
            pltpu.VMEM((ranks, 2, channels, width), BF16),
            pltpu.VMEM((heads * tp * VD, width), BF16),
            pltpu.VMEM((max(ranks - 1, 1), tok, width), BF16),
            pltpu.VMEM((max(ranks - 1, 1), tok, width), BF16),
            pltpu.VMEM((tok, heads * tp * VD), BF16),
            pltpu.VMEM((tok, width), F32),
            pltpu.VMEM((tok, width), BF16),
            pltpu.VMEM((tp, 8, tok), F32),
            dma,
            dma,
            dma((RING,)),
            dma((n,)),
            dma((n,)),
            dma((n,)),
            dma((n,)),
            dma((n,)),
            dma((n,)),
            dma((n,)),
            dma((n,)),
            dma((3,)),
            dma((3,)),
            dma((tp, heads)),
            dma((tp, heads)),
            dma((tp, heads)),
            dma((ranks,)),
            dma((ranks,)),
            dma((ranks,)),
            dma((ranks, tok // SPAN)),
            dma((ranks, tok // SPAN)),
            dma((ranks, n)),
            dma((ranks, n)),
            dma((ranks, n)),
            dma((ranks, n)),
            dma((tp,)),
            dma((tp,)),
            dma((tok // SPAN,)),
        ],
        compiler_params=pltpu.CompilerParams(
            vmem_limit_bytes=VMEM_LIMIT, collective_id=0, has_side_effects=True
        ),
        cost_estimate=pl.CostEstimate(
            flops=12 * tok * model * channels + 4 * n * n * rows * tok * VD,
            bytes_accessed=2 * model * (tok + 6 * channels),
            transcendentals=0,
        ),
        name="mixer",
    )(
        jnp.asarray(turn),
        jnp.asarray(base),
        conv_taps,
        lambdas,
        head_gain[None],
        hidden_states,
        w_query,
        w_key,
        w_value,
        w_conv_b,
        w_conv_c,
        w_conv_h,
        w_out_conv,
        w_out_attn,
    )
    own_gain = lax.dynamic_slice_in_dim(out_gain, lax.axis_index("tp") * width, width, 0)
    grid = tok // SPAN
    return pl.pallas_call(
        scale_kernel,
        grid=(grid,),
        out_shape=jax.ShapeDtypeStruct((tok, width), BF16),
        in_specs=[
            pl.BlockSpec((SPAN, width), lambda i: (i, 0)),
            pl.BlockSpec((8, SPAN), lambda i: (0, i)),
            pl.BlockSpec((1, width), lambda i: (0, 0)),
        ],
        out_specs=pl.BlockSpec((SPAN, width), lambda i: (i, 0)),
        cost_estimate=pl.CostEstimate(
            flops=4 * tok * width, bytes_accessed=4 * tok * width, transcendentals=0
        ),
        name="scale",
    )(mix, stat, own_gain.astype(F32)[None, :])


def solution(mesh):
    n, tp = mesh.shape["sp"], mesh.shape["tp"]
    return jax.shard_map(
        functools.partial(per_device, n, tp),
        mesh=mesh,
        in_specs=(
            P("sp", None),
            P(None, "tp"),
            P(None, "tp"),
            P(None, "tp"),
            P(None, "tp"),
            P(None, "tp"),
            P(None, "tp"),
            P(None, "tp"),
            P("tp"),
            P(),
            P("tp", None),
            P("tp", None),
            P(),
        ),
        out_specs=P("sp", "tp"),
        check_vma=False,
    )
```

```python
import functools
import math

import jax
import jax.numpy as jnp
import numpy as np
from jax import lax
from jax.experimental import pallas as pl
from jax.experimental.pallas import tpu as pltpu
from jax.sharding import PartitionSpec as P

QK = 64
VD = 128
TILE = 256
SPAN = 256
RIM = 16
RING = 4
NEG_LARGE = -1e30
VMEM_LIMIT = 67_000_000
MESH = pl.DeviceIdType.MESH
BF16, F32 = jnp.bfloat16, jnp.float32


def mixer_kernel(
    n,
    tp,
    turn_ref,
    base_hbm,
    taps_hbm,
    lam_ref,
    gain_hbm,
    x_hbm,
    wq_ref,
    wk_ref,
    wv_ref,
    wb_ref,
    wc_ref,
    wh_ref,
    w_conv_ref,
    w_attn_ref,
    out_ref,
    stat_ref,
    x_ref,
    cos_ref,
    sin_ref,
    tables,
    wbuf,
    raw_ref,
    q_own,
    kv_own,
    q_all,
    kv_all,
    out_own,
    m_ref,
    l_ref,
    acc_ref,
    lam_all,
    rim_x,
    rim_raw,
    conv_chip,
    wc_all,
    wa_all,
    part_out,
    part_in,
    attn_all,
    total_ref,
    mix_ref,
    stats,
    base_ref,
    taps_ref,
    gain_ref,
    x_sem,
    turn_sem,
    tiny_sem,
    w_sem,
    send_q,
    send_kv,
    recv_q,
    recv_kv,
    send_fwd,
    recv_fwd,
    send_o,
    recv_o,
    small_send,
    small_recv,
    send_wa,
    recv_wa,
    send_wf,
    send_wc,
    recv_wc,
    local_wc,
    send_part,
    recv_part,
    send_y,
    recv_y,
    send_s,
    recv_s,
    send_stat,
    recv_stat,
    mix_sem,
):
    j, t = lax.axis_index("sp"), lax.axis_index("tp")
    c, y = t % 2, t // 2
    ranks = tp // 2
    tok, model = x_ref.shape
    width = model // tp
    heads = q_own.shape[0]
    channels = wc_all.shape[2]
    half = n // 2
    repeat = half // heads
    parts = 2 * repeat
    rows = tok // parts
    per = TILE // VD
    pairs, tiles = heads // per, channels // TILE

    def remote(src, dst, send_sem, recv_sem, device):
        return pltpu.make_async_remote_copy(
            src_ref=src,
            dst_ref=dst,
            send_sem=send_sem,
            recv_sem=recv_sem,
            device_id=device,
            device_id_type=MESH,
        )

    sibling = (j, y * 2 + 1 - c)

    def peer(step):
        return (j, (y + step) % ranks * 2 + c)

    barrier = pltpu.get_barrier_semaphore()
    x_copy = pltpu.make_async_copy(x_hbm, x_ref, x_sem)
    x_copy.start()

    turn_copy = pltpu.make_async_copy(turn_ref, tables, turn_sem)
    turn_copy.start()
    tiny = [
        pltpu.make_async_copy(src, dst, tiny_sem.at[i])
        for i, (src, dst) in enumerate(
            ((base_hbm, base_ref), (taps_hbm, taps_ref), (gain_hbm, gain_ref))
        )
    ]
    for copy in tiny:
        copy.start()
    products = 3 * (pairs + tiles)
    side = j // half
    early = c == side
    shift = jnp.where(jnp.logical_and(side == 1, c == 0), 0, 1)
    lead = jnp.where(early, 0, tiles)

    def product(i):
        is_conv = jnp.logical_or(i < lead, i >= lead + 3 * pairs)
        r = jnp.where(i < lead, i, i - 3 * pairs)
        q = i - lead
        gate = r < tiles
        conv_kind = jnp.where(gate, 3, 4 + (r - tiles) % 2)
        conv_index = jnp.where(gate, r, (r - tiles) // 2)
        kind = jnp.where(is_conv, conv_kind, (q // pairs + shift) % 3)
        index = jnp.where(is_conv, conv_index, (q % pairs + j) % pairs)
        return kind, index

    def load(i):
        kind, index = product(i)
        for w, ref in enumerate((wq_ref, wk_ref, wv_ref, wb_ref, wc_ref, wh_ref)):

            @pl.when(kind == w)
            def _():
                pltpu.make_async_copy(
                    ref.at[:, pl.ds(pl.multiple_of(index * TILE, TILE), TILE)],
                    wbuf.at[i % RING],
                    w_sem.at[i % RING],
                ).start()

    load(0)

    @pl.loop(0, n)
    def _(a):
        for e in range(2):

            @pl.when(jnp.logical_or(a != j, c != e))
            def _():
                pl.semaphore_signal(
                    barrier, inc=1, device_id=(a, y * 2 + e), device_id_type=MESH
                )

    @pl.loop(1, ranks)
    def _(step):
        for e in range(2):
            pl.semaphore_signal(
                barrier,
                inc=1,
                device_id=(j, (y + step) % ranks * 2 + e),
                device_id_type=MESH,
            )

    for copy in tiny:
        copy.wait()
    lane_row = lax.broadcasted_iota(jnp.int32, (1, VD), 1)
    cos_far, sin_far = base_ref[0, pl.ds(j, 1)], base_ref[1, pl.ds(j, 1)]
    turn_copy.wait()
    cos_ref[...] = cos_far * tables[0] - sin_far * tables[1]
    sin_ref[...] = jnp.where(lane_row % QK < QK // 2, -1.0, 1.0) * (
        sin_far * tables[0] + cos_far * tables[1]
    )
    for i in range(1, RING - 1):
        load(i)
    for h in range(heads):
        lam_all[c, h : h + 1] = jnp.full((1, VD), lam_ref[h], F32)

    rim_copy = remote(
        x_ref.at[pl.ds(tok - RIM, RIM)],
        rim_x,
        small_send.at[1],
        small_recv.at[1],
        (jnp.minimum(j + 1, n - 1), t),
    )
    lam_copy = remote(lam_all.at[c], lam_all.at[c], small_send.at[0], small_recv.at[0], sibling)

    def place(head, source):
        order = source % 2 * ranks + source // 2
        return pl.multiple_of((head * tp + order) * VD, VD)

    def wa_rows(head, source):
        return wa_all.at[pl.ds(place(head, source), VD)]

    def wa_block(head, target):
        return w_attn_ref.at[
            pl.ds(pl.multiple_of(head * VD, VD), VD),
            pl.ds(pl.multiple_of(target * width, VD), width),
        ]

    def wc_cols(rank, core):
        return w_conv_ref.at[:, pl.ds(pl.multiple_of((rank * 2 + core) * width, VD), width)]

    direct = heads // 2
    passed = heads - direct
    odd = j % 2
    first_direct, first_passed, first_lacking = odd * passed, odd * direct, (1 - odd) * direct

    def local_weights():
        for head in range(heads):
            pltpu.make_async_copy(
                wa_block(head, t), wa_rows(head, t), recv_wa.at[t, head]
            ).start()

        @pl.loop(0, ranks)
        def _(rank):
            pltpu.make_async_copy(wc_cols(rank, c), wc_all.at[rank, c], local_wc.at[rank]).start()

    def early_sends():
        pl.semaphore_wait(barrier, 2 * n - 1 + 2 * (ranks - 1))

        @pl.when(j + 1 < n)
        def _():
            rim_copy.start()

        lam_copy.start()

        @pl.loop(1, ranks)
        def _(step):
            for e in range(2):
                target = (y + step) % ranks * 2 + e
                for h in range(direct):
                    head = first_direct + h
                    remote(
                        wa_block(head, target),
                        wa_rows(head, t),
                        send_wa.at[target, head],
                        recv_wa.at[t, head],
                        (j, target),
                    ).start()

    def sibling_weights():
        for head in range(heads):
            target = y * 2 + 1 - c
            remote(
                wa_block(head, target),
                wa_rows(head, t),
                send_wa.at[target, head],
                recv_wa.at[t, head],
                sibling,
            ).start()

        @pl.loop(0, ranks)
        def _(rank):
            remote(
                wc_cols(rank, 1 - c),
                wc_all.at[rank, c],
                send_wc.at[rank],
                recv_wc.at[rank],
                sibling,
            ).start()

    def pass_weights():
        @pl.loop(1, ranks)
        def _(step):
            for e in range(2):
                source = (y + step) % ranks * 2 + e
                for h in range(passed):
                    head = first_passed + h
                    block = wa_rows(head, source)
                    arrived(block, recv_wa.at[source, head])
                    remote(
                        block,
                        block,
                        send_wf.at[source, h],
                        recv_wa.at[source, head],
                        (j + 1 - 2 * odd, t),
                    ).start()

    def part_of(block, rep, core):
        part = rep * 2 + core
        return jnp.where(block % 2 == 0, part, parts - 1 - part)

    def put(src, dst, send_sem, recv_sem, device, here):
        @pl.when(here)
        def _():
            pltpu.make_async_copy(src, dst, recv_sem).start()

        @pl.when(jnp.logical_not(here))
        def _():
            remote(src, dst, send_sem, recv_sem, device).start()

    def sent(src, send_sem):
        remote(src, src, send_sem, send_sem, sibling).wait_send()

    def put_done(src, send_sem, here):
        @pl.when(jnp.logical_not(here))
        def _():
            sent(src, send_sem)

    def arrived(dst, recv_sem):
        pltpu.make_async_copy(dst, dst, recv_sem).wait()

    lane = lax.broadcasted_iota(jnp.int32, (tok, VD), 1)
    low = lane % QK < QK // 2
    fold = QK ** (-0.5) * math.log2(math.e)

    def rotate(values):
        values = values.astype(F32)
        partner = jnp.where(
            low, pltpu.roll(values, VD - QK // 2, 1), pltpu.roll(values, QK // 2, 1)
        )
        return values * cos_ref[...] + partner * sin_ref[...]

    def send_kv_of(e, pair):
        for p in range(per):
            head = pair * per + p
            for r in range(repeat):
                local = head * repeat + r
                s = c * half + local
                put(
                    kv_own.at[e, head],
                    kv_all.at[e, j],
                    send_kv.at[local * 2 + e],
                    recv_kv.at[j],
                    (s, y * 2 + e),
                    jnp.logical_and(s == j, c == e),
                )

    def send_q_of(pair):
        for p in range(per):
            head = pair * per + p
            for r in range(repeat):
                local = head * repeat + r
                s = c * half + local
                for e in range(2):
                    first = pl.multiple_of(part_of(j, r, e) * rows, 16)
                    put(
                        q_own.at[head, pl.ds(first, rows)],
                        q_all.at[j],
                        send_q.at[local * 2 + e],
                        recv_q.at[j],
                        (s, y * 2 + e),
                        jnp.logical_and(s == j, c == e),
                    )

    def convolve(g):
        cols = pl.ds(pl.multiple_of(g * TILE, TILE), TILE)
        gated = raw_ref[1].astype(F32) * raw_ref[2].astype(F32)
        before = jnp.where(j > 0, rim_raw[0] * rim_raw[1], 0.0)
        one, two = before[RIM - 1 :], before[RIM - 2 : RIM - 1]
        row = lax.broadcasted_iota(jnp.int32, gated.shape, 0)
        back_one = jnp.where(row == 0, one, pltpu.roll(gated, 1, 0))
        back_two = jnp.where(row == 0, two, jnp.where(row == 1, one, pltpu.roll(gated, 2, 0)))
        tap = taps_ref[:, cols].astype(F32)
        conv = tap[0:1] * back_two + tap[1:2] * back_one + tap[2:3] * gated
        conv_chip[c, :, cols] = (raw_ref[3 + g].astype(F32) * conv).astype(BF16)


    def forward(block):
        here = kv_all.at[c, block]
        arrived(here, recv_kv.at[block])
        remote(here, here, send_fwd.at[block], recv_fwd.at[block], sibling).start()

    def keys_sent(first):
        @pl.loop(0, half)
        def _(b):
            forward(first + b)

    conv_copy = remote(
        conv_chip.at[c], conv_chip.at[c], small_send.at[2], small_recv.at[2], sibling
    )

    def conv_product(first, rank):
        span = pl.ds(first, SPAN)
        return jnp.dot(
            conv_chip[0, span], wc_all[rank, 0], preferred_element_type=F32
        ) + jnp.dot(conv_chip[1, span], wc_all[rank, 1], preferred_element_type=F32)

    def conv_parts():
        conv_copy.wait_recv()

        @pl.loop(0, ranks)
        def _(rank):
            mine = wc_all.at[rank, c]
            theirs = wc_all.at[rank, 1 - c]
            arrived(mine, local_wc.at[rank])
            arrived(theirs, recv_wc.at[rank])

        @pl.loop(1, ranks)
        def _(step):
            @pl.loop(0, tok // SPAN)
            def _(b):
                first = pl.multiple_of(b * SPAN, SPAN)
                span = pl.ds(first, SPAN)
                part_out[step - 1, span] = conv_product(first, (y + step) % ranks).astype(BF16)
                remote(
                    part_out.at[step - 1, span],
                    part_in.at[step - 1, span],
                    send_part.at[step - 1, b],
                    recv_part.at[step - 1, b],
                    peer(step),
                ).start()

    x_copy.wait()

    @pl.loop(0, products)
    def _(i):
        kind, index = product(i)

        @pl.when(i + RING - 1 < products)
        def _():
            load(i + RING - 1)

        arrived(wbuf.at[i % RING], w_sem.at[i % RING])
        raw_ref[jnp.where(kind == 3, 3 + index, kind % 3)] = jnp.dot(
            x_ref[...], wbuf[i % RING], preferred_element_type=F32
        ).astype(BF16)

        @pl.when(i == 0)
        def _():
            early_sends()

        @pl.when(jnp.logical_and(kind >= 4, j > 0))
        def _():
            @pl.when(jnp.logical_and(kind == 4, index == 0))
            def _():
                rim_copy.wait_recv()

            rim_raw[kind - 4] = (
                jnp.dot(rim_x[...], wbuf[i % RING], preferred_element_type=F32)
                .astype(BF16)
                .astype(F32)
            )

        @pl.when(i == 2)
        def _():
            local_weights()
            sibling_weights()

        @pl.when(kind == 1)
        def _():
            for p in range(per):
                kv_own[0, index * per + p] = rotate(
                    raw_ref[1, :, p * VD : (p + 1) * VD]
                ).astype(BF16)
            send_kv_of(0, index)

        @pl.when(kind == 2)
        def _():
            for p in range(per):
                kv_own[1, index * per + p] = raw_ref[2, :, p * VD : (p + 1) * VD]
            send_kv_of(1, index)

        @pl.when(kind == 0)
        def _():
            for p in range(per):
                q_own[index * per + p] = (
                    rotate(raw_ref[0, :, p * VD : (p + 1) * VD]) * fold
                ).astype(BF16)
            send_q_of(index)

        @pl.when(kind == 5)
        def _():
            convolve(index)

    lam_copy.wait()
    conv_copy.start()
    keys_sent(side * half)
    conv_parts()
    pass_weights()

    head_at = (j % half) // repeat
    rep_at = j % repeat
    owner_tp = y * 2 + side
    lam = lam_all[side, pl.ds(head_at, 1)]
    gain = gain_ref[...].astype(F32)
    block_lane = lax.broadcasted_iota(jnp.int32, (rows, VD), 1)

    def scores(both, kb, part, masked):
        s = lax.dot_general(
            both, kv_all[0, kb], (((1,), (1,)), ((), ())), preferred_element_type=F32
        )
        if masked:
            r = part * rows + lax.broadcasted_iota(jnp.int32, s.shape, 0) % rows
            s = jnp.where(lax.broadcasted_iota(jnp.int32, s.shape, 1) <= r, s, NEG_LARGE)
        return s

    def attend(slot, both, part, jobs):
        ahead = scores(both, jobs[0][0], part, jobs[0][1])
        for number, (kb, _) in enumerate(jobs):
            s = ahead
            if number + 1 < len(jobs):
                ahead = scores(both, jobs[number + 1][0], part, jobs[number + 1][1])
            weigh(slot, s, kv_all[1, kb])

    def weigh(slot, s, v):
        slabs = [s[:, b * VD : (b + 1) * VD] for b in range(tok // VD)]
        old = m_ref[slot]
        top = functools.reduce(jnp.maximum, slabs)
        new = jnp.maximum(old, jnp.max(top, axis=1, keepdims=True))
        factor = jnp.exp2(old - new)
        total = l_ref[slot] * factor
        weights = []
        for slab in slabs:
            w = jnp.exp2(slab - new)
            total = total + w
            weights.append(w.astype(BF16))
        m_ref[slot] = new
        l_ref[slot] = total
        acc_ref[slot] = acc_ref[slot] * factor + jnp.dot(
            jnp.concatenate(weights, axis=1), v, preferred_element_type=F32
        )

    def piece(head, source, part):
        return attn_all.at[
            pl.ds(pl.multiple_of(part * rows, 16), rows),
            pl.ds(place(head, source), VD),
        ]

    def piece_of(k, core, source):
        local = (j - k) % half
        head, rep = local // repeat, local % repeat
        return local * 2 + core, piece(head, source, part_of(j, rep, core))

    def share(k):
        for core in range(2):
            index, mine = piece_of(k, core, t)
            arrived(mine, recv_o.at[index])

            @pl.loop(1, ranks)
            def _(step):
                remote(
                    mine, mine, send_y.at[step, index], recv_y.at[step, index], peer(step)
                ).start()

            remote(mine, mine, send_s.at[y, index], recv_s.at[y, index], sibling).start()

    def relay(k):
        @pl.loop(1, ranks)
        def _(step):
            rank = (y + ranks - step) % ranks
            for core in range(2):
                index, theirs = piece_of(k, core, rank * 2 + c)
                arrived(theirs, recv_y.at[step, index])
                remote(
                    theirs, theirs, send_s.at[rank, index], recv_s.at[rank, index], sibling
                ).start()

    def gathered(k):
        @pl.loop(0, ranks)
        def _(rank):
            for core in range(2):
                index, theirs = piece_of(k, core, rank * 2 + 1 - c)
                arrived(theirs, recv_s.at[rank, index])

    def own_product():
        @pl.loop(1, ranks)
        def _(step):
            @pl.loop(0, tok // SPAN)
            def _(b):
                arrived(part_in.at[step - 1, pl.ds(0, SPAN)], recv_part.at[step - 1, b])

        @pl.loop(0, tok // SPAN)
        def _(b):
            first = pl.multiple_of(b * SPAN, SPAN)
            value = conv_product(first, y)
            for step in range(1, ranks):
                value = value + part_in[step - 1, pl.ds(first, SPAN)].astype(F32)
            total_ref[pl.ds(first, SPAN)] = value

    @pl.loop(0, 3 * half)
    def _(step):
        phase = step // half
        turn = (step + j) % half
        group = jnp.where(phase == 0, side, jnp.where(phase == 1, 1, 1 - side))
        block = group * half + turn
        base = group * half
        slot = jnp.where(group == 0, half, turn)
        enter = step % half == 0
        other = (1 - side) * half

        def keys_ready(first):
            @pl.loop(0, half)
            def _(b):
                arrived(kv_all.at[1 - c, first + b], recv_fwd.at[first + b])

        def queries_ready(first):
            @pl.loop(0, half)
            def _(b):
                arrived(q_all.at[first + b], recv_q.at[first + b])

        @pl.when(jnp.logical_and(enter, phase == 0))
        def _():
            keys_ready(base)
            queries_ready(base)

        @pl.when(jnp.logical_and(enter, phase == 1 + side))
        def _():
            queries_ready(other)

        @pl.when(step == jnp.where(side == 0, 2 * half - 1, half))
        def _():
            keys_sent(other)

        @pl.when(jnp.logical_and(enter, phase == 2 - side))
        def _():
            keys_ready(other)

        @pl.when(step == 2 * half + 2)
        def _():
            own_product()

        @pl.when(jnp.logical_and(early, step == 2 * half + 1))
        def _():
            @pl.loop(0, half)
            def _(k):
                share(k)

        @pl.when(jnp.logical_and(early, step == 2 * half + 3))
        def _():
            @pl.loop(0, half)
            def _(k):
                relay(k)

        @pl.when(jnp.logical_and(jnp.logical_not(early), step > 2 * half + 2))
        def _():
            share(step - 2 * half - 3)

        q = q_all[block]
        zero = jnp.zeros_like(q)
        both = jnp.concatenate(
            [jnp.where(block_lane < QK, q, zero), jnp.where(block_lane < QK, zero, q)], axis=0
        )
        part = part_of(block, rep_at, c)

        @pl.when(phase == jnp.where(group == 0, phase, 1 - side))
        def _():
            m_ref[slot] = jnp.full(m_ref.shape[1:], NEG_LARGE, F32)
            l_ref[slot] = jnp.zeros(l_ref.shape[1:], F32)
            acc_ref[slot] = jnp.zeros(acc_ref.shape[1:], F32)

        low_kb = jnp.where(phase == 1, 0, base)
        count = jnp.where(phase == 1, half, block - base)

        @pl.loop(0, count // 2)
        def _(p):
            kb = low_kb + 2 * p
            attend(slot, both, part, [(kb, False), (kb + 1, False)])

        @pl.when(jnp.logical_and(phase != 1, count % 2 == 1))
        def _():
            attend(slot, both, part, [(block - 1, False), (block, True)])

        @pl.when(jnp.logical_and(phase != 1, count % 2 == 0))
        def _():
            attend(slot, both, part, [(block, True)])

        @pl.when(phase >= jnp.where(group == 0, 0, 2 - side))
        def _():
            first, second = (
                acc_ref[slot, span] / jnp.sum(l_ref[slot, span], axis=1, keepdims=True)
                for span in (pl.ds(0, rows), pl.ds(rows, rows))
            )
            diff = first - lam * second
            norm = lax.rsqrt(jnp.mean(diff * diff, axis=1, keepdims=True) + 1e-05)
            out_own[block] = (diff * norm * gain).astype(BF16)
            put(
                out_own.at[block],
                piece(head_at, owner_tp, part),
                send_o.at[block],
                recv_o.at[(j % half) * 2 + c],
                (block, owner_tp),
                jnp.logical_and(block == j, side == c),
            )

    for head in range(heads):
        for e in range(2):
            source = y * 2 + e
            arrived(wa_rows(head, source), recv_wa.at[source, head])

    @pl.loop(1, ranks)
    def _(step):
        for e in range(2):
            source = (y + step) % ranks * 2 + e
            for h in range(passed):
                head = first_lacking + h
                arrived(wa_rows(head, source), recv_wa.at[source, head])
            for h in range(direct - passed):
                head = passed + h
                arrived(wa_rows(head, source), recv_wa.at[source, head])

    def accumulate(k, group):
        @pl.when(c != group)
        def _():
            gathered(k)

        local = (j - k) % half
        head, rep = local // repeat, local % repeat
        deep = pl.ds(place(head, group), ranks * VD)
        for core in range(2):
            span = pl.ds(pl.multiple_of(part_of(j, rep, core) * rows, 16), rows)
            total_ref[span] = total_ref[span] + jnp.dot(
                attn_all[span, deep], wa_all[deep], preferred_element_type=F32
            )

    @pl.loop(0, half)
    def _(k):
        accumulate(k, side)

    @pl.when(jnp.logical_not(early))
    def _():
        @pl.loop(half - 3, half)
        def _(k):
            share(k)

        @pl.loop(0, half)
        def _(k):
            relay(k)

    @pl.loop(0, half)
    def _(k):
        accumulate(k, 1 - side)

    slabs = width // VD

    def mix_copy(b):
        span = pl.ds(pl.multiple_of(b * SPAN, SPAN), SPAN)
        return pltpu.make_async_copy(mix_ref.at[span], out_ref.at[span], mix_sem.at[b])

    @pl.loop(0, tok // SPAN)
    def _(b):
        span = pl.ds(pl.multiple_of(b * SPAN, SPAN), SPAN)
        mix = total_ref[span].astype(BF16)
        mix_ref[span] = mix
        mix_copy(b).start()
        sums = jnp.zeros((SPAN, VD), F32)
        squares = jnp.zeros((SPAN, VD), F32)
        for s in range(slabs):
            slab = mix[:, s * VD : (s + 1) * VD].astype(F32)
            sums = sums + slab
            squares = squares + slab * slab
        stats[t, 0:1, span] = jnp.sum(sums.T, axis=0, keepdims=True)
        stats[t, 1:2, span] = jnp.sum(squares.T, axis=0, keepdims=True)

    def stat_copy(step):
        return remote(
            stats.at[t],
            stats.at[t],
            send_stat.at[step],
            recv_stat.at[step],
            (j, (t + step) % tp),
        )

    @pl.loop(1, tp)
    def _(step):
        stat_copy(step).start()

    @pl.loop(1, tp)
    def _(step):
        source = (t + tp - step) % tp
        arrived(stats.at[source], recv_stat.at[step])

    @pl.loop(0, tok // SPAN)
    def _(b):
        span = pl.ds(pl.multiple_of(b * SPAN, SPAN), SPAN)
        sums, squares = stats[0, 0:1, span], stats[0, 1:2, span]
        for source in range(1, tp):
            sums = sums + stats[source, 0:1, span]
            squares = squares + stats[source, 1:2, span]
        mean = sums / model
        scale = lax.rsqrt(squares / model - mean * mean + 1e-05)
        stat_ref[0:1, span] = mean
        stat_ref[1:2, span] = scale


    @pl.loop(0, tok // SPAN)
    def _(b):
        mix_copy(b).wait()

    @pl.when(j + 1 < n)
    def _():
        rim_copy.wait_send()

    conv_copy.wait_send()

    @pl.loop(0, half)
    def _(local):
        head = local // repeat
        s = c * half + local
        for e in range(2):
            here = jnp.logical_and(s == j, c == e)
            put_done(kv_own.at[e, head], send_kv.at[local * 2 + e], here)
            put_done(q_own.at[head, pl.ds(0, rows)], send_q.at[local * 2 + e], here)

    @pl.loop(0, n)
    def _(block):
        sent(kv_all.at[c, block], send_fwd.at[block])
        put_done(out_own.at[block], send_o.at[block], jnp.logical_and(block == j, side == c))

        @pl.loop(1, ranks)
        def _(step):
            sent(out_own.at[0], send_y.at[step, block])

        @pl.loop(0, ranks)
        def _(rank):
            sent(out_own.at[0], send_s.at[rank, block])

    @pl.loop(1, tp)
    def _(step):
        stat_copy(step).wait_send()

    for head in range(heads):
        sent(wa_rows(head, t), send_wa.at[y * 2 + 1 - c, head])

    @pl.loop(1, ranks)
    def _(step):
        for e in range(2):
            other = (y + step) % ranks * 2 + e
            for h in range(direct):
                sent(wa_rows(h, t), send_wa.at[other, first_direct + h])
            for h in range(passed):
                sent(wa_rows(h, t), send_wf.at[other, h])

    @pl.loop(0, ranks)
    def _(rank):
        sent(wc_all.at[rank, c], send_wc.at[rank])

    @pl.loop(1, ranks)
    def _(step):
        @pl.loop(0, tok // SPAN)
        def _(b):
            sent(part_out.at[step - 1, pl.ds(0, SPAN)], send_part.at[step - 1, b])


def scale_kernel(mix_ref, stat_ref, gain_ref, out_ref):
    rows, width = mix_ref.shape
    first = lax.axis_index("tp") * width
    mean = jnp.broadcast_to(stat_ref[0:1], (VD, rows)).T
    scale = jnp.broadcast_to(stat_ref[1:2], (VD, rows)).T
    for s in range(width // VD):
        cols = slice(s * VD, (s + 1) * VD)
        value = (mix_ref[:, cols].astype(F32) - mean) * scale
        if s % 2 == 0:
            at = pl.multiple_of(first + s * VD, 2 * VD)
            gain = gain_ref[pl.ds(at, 2 * VD)].astype(F32).reshape(1, 2 * VD)
        part = gain[:, s % 2 * VD : (s % 2 + 1) * VD]
        out_ref[:, cols] = (value * part).astype(BF16)


def per_device(
    n,
    tp,
    hidden_states,
    w_conv_b,
    w_conv_c,
    w_conv_h,
    conv_taps,
    w_query,
    w_key,
    w_value,
    lambdas,
    head_gain,
    w_out_conv,
    w_out_attn,
    out_gain,
):
    tok, model = hidden_states.shape
    heads = w_value.shape[1] // VD
    channels = w_conv_b.shape[1]
    half = n // 2
    repeat = half // heads
    parts = 2 * repeat
    rows = tok // parts
    ranks = tp // 2
    width = model // tp

    inverse = 10000.0 ** (-np.arange(0, QK, 2, dtype=np.float64) / QK)
    inverse = np.tile(inverse, VD // inverse.size)[None, :]
    table = lambda angles: np.stack([np.cos(angles), np.sin(angles)]).astype(np.float32)
    turn = table(np.arange(tok)[:, None] * inverse)
    base = table(np.arange(n)[:, None] * tok * inverse)
    lam_rows = -(-heads // 8) * 8

    vmem, hbm = pl.BlockSpec(memory_space=pltpu.VMEM), pl.BlockSpec(memory_space=pl.ANY)
    smem = pl.BlockSpec(memory_space=pltpu.SMEM)
    dma = pltpu.SemaphoreType.DMA
    mix, stat = pl.pallas_call(
        functools.partial(mixer_kernel, n, tp),
        out_shape=(
            jax.ShapeDtypeStruct((tok, width), BF16),
            jax.ShapeDtypeStruct((8, tok), F32),
        ),
        in_specs=[hbm] * 3 + [smem] + [hbm] * 10,
        out_specs=(hbm, vmem),
        scratch_shapes=[
            pltpu.VMEM((tok, model), BF16),
            pltpu.VMEM((tok, VD), F32),
            pltpu.VMEM((tok, VD), F32),
            pltpu.VMEM((2, tok, VD), F32),
            pltpu.VMEM((RING, model, TILE), BF16),
            pltpu.VMEM((3 + channels // TILE, tok, TILE), BF16),
            pltpu.VMEM((heads, tok, VD), BF16),
            pltpu.VMEM((2, heads, tok, VD), BF16),
            pltpu.VMEM((n, rows, VD), BF16),
            pltpu.VMEM((2, n, tok, VD), BF16),
            pltpu.VMEM((n, rows, VD), BF16),
            pltpu.VMEM((half + 1, 2 * rows, VD), F32),
            pltpu.VMEM((half + 1, 2 * rows, VD), F32),
            pltpu.VMEM((half + 1, 2 * rows, VD), F32),
            pltpu.VMEM((2, lam_rows, VD), F32),
            pltpu.VMEM((RIM, model), BF16),
            pltpu.VMEM((2, RIM, TILE), F32),
            pltpu.VMEM((2, tok, channels), BF16),
            pltpu.VMEM((ranks, 2, channels, width), BF16),
            pltpu.VMEM((heads * tp * VD, width), BF16),
            pltpu.VMEM((max(ranks - 1, 1), tok, width), BF16),
            pltpu.VMEM((max(ranks - 1, 1), tok, width), BF16),
            pltpu.VMEM((tok, heads * tp * VD), BF16),
            pltpu.VMEM((tok, width), F32),
            pltpu.VMEM((tok, width), BF16),
            pltpu.VMEM((tp, 8, tok), F32),
            pltpu.VMEM((2, n, VD), F32),
            pltpu.VMEM(conv_taps.shape, BF16),
            pltpu.VMEM((1, VD), BF16),
            dma,
            dma,
            dma((3,)),
            dma((RING,)),
            dma((n,)),
            dma((n,)),
            dma((n,)),
            dma((n,)),
            dma((n,)),
            dma((n,)),
            dma((n,)),
            dma((n,)),
            dma((3,)),
            dma((3,)),
            dma((tp, heads)),
            dma((tp, heads)),
            dma((tp, heads)),
            dma((ranks,)),
            dma((ranks,)),
            dma((ranks,)),
            dma((ranks, tok // SPAN)),
            dma((ranks, tok // SPAN)),
            dma((ranks, n)),
            dma((ranks, n)),
            dma((ranks, n)),
            dma((ranks, n)),
            dma((tp,)),
            dma((tp,)),
            dma((tok // SPAN,)),
        ],
        compiler_params=pltpu.CompilerParams(
            vmem_limit_bytes=VMEM_LIMIT, collective_id=0, has_side_effects=True
        ),
        cost_estimate=pl.CostEstimate(
            flops=12 * tok * model * channels + 4 * n * n * rows * tok * VD,
            bytes_accessed=2 * model * (tok + 6 * channels),
            transcendentals=0,
        ),
        name="mixer",
    )(
        jnp.asarray(turn),
        jnp.asarray(base),
        conv_taps,
        lambdas,
        head_gain[None],
        hidden_states,
        w_query,
        w_key,
        w_value,
        w_conv_b,
        w_conv_c,
        w_conv_h,
        w_out_conv,
        w_out_attn,
    )
    grid = tok // SPAN
    return pl.pallas_call(
        scale_kernel,
        grid=(grid,),
        out_shape=jax.ShapeDtypeStruct((tok, width), BF16),
        in_specs=[
            pl.BlockSpec((SPAN, width), lambda i: (i, 0)),
            pl.BlockSpec((8, SPAN), lambda i: (0, i)),
            pl.BlockSpec((model,), lambda i: (0,)),
        ],
        out_specs=pl.BlockSpec((SPAN, width), lambda i: (i, 0)),
        cost_estimate=pl.CostEstimate(
            flops=4 * tok * width, bytes_accessed=4 * tok * width, transcendentals=0
        ),
        name="scale",
    )(mix, stat, out_gain)


def solution(mesh):
    n, tp = mesh.shape["sp"], mesh.shape["tp"]
    return jax.shard_map(
        functools.partial(per_device, n, tp),
        mesh=mesh,
        in_specs=(
            P("sp", None),
            P(None, "tp"),
            P(None, "tp"),
            P(None, "tp"),
            P(None, "tp"),
            P(None, "tp"),
            P(None, "tp"),
            P(None, "tp"),
            P("tp"),
            P(),
            P("tp", None),
            P("tp", None),
            P(),
        ),
        out_specs=P("sp", "tp"),
        check_vma=False,
    )
```
